128 devices in a mesh: fs: 16 (over z, y), tp: 8 (over x, core).
Axes of the slice: x: 4, y: 4, z: 4, core: 2. Of those that a mesh axis runs over, the one named last changes fastest.
Arguments:
- tokens: bfloat16 [16384, 2048], P('fs', 'tp'), may hold values from -6 to 6
- norm_gain: float32 [2048], P('fs'), may hold values from 0.1 to 1.9
- up_master: float32 [2048, 8192], P('fs', 'tp'), may hold values from -0.125 to 0.125
- down_master: float32 [2048, 8192], P('fs', 'tp'), may hold values from -0.0625 to 0.0625
Outputs:
- up_weights: bfloat16 [2048, 8192], P(None, 'tp')
- down_weights: bfloat16 [8192, 2048], P('tp')
- mlp_out: bfloat16 [16384, 2048], P('fs', 'tp')
The draws below stay inside these ranges and needn't reach their ends.
All inputs are finite; a program needn't handle non-finite values.
Results may differ from the reference program's by a relative error of at most 0.014.
Values may be sent and summed in bfloat16 or wider, within the bound.
A program may use at most 128 MiB of HBM per device.

```python
import jax
import jax.numpy as jnp
from jax import lax

D = 2048
FF = 8192
TOKENS = 16384
N_TP = 8


def block_scale(key, extent, cuts, smallest, high):
    loudness = 1.0
    for axis_at, parts in cuts:
        draws = jax.random.uniform(jax.random.fold_in(jax.random.fold_in(key, 6), axis_at), (parts,), jnp.float32, smallest / len(cuts), high / len(cuts))
        loudness = loudness * jnp.repeat(jnp.exp(draws), extent[axis_at] // parts).reshape((-1,) + (1,) * (len(extent) - 1 - axis_at))
    return loudness


def bell_draw(stream_key, shape, width, limit, shards=(), held_as=jnp.bfloat16):
    result = jax.random.normal(stream_key, shape, jnp.float32) * width
    if len(shards) > 0:
        result = block_scale(stream_key, shape, shards, -0.22, 0.18) * result
    return jnp.clip(result, min=-limit, max=limit).astype(held_as)


def setup_inputs(seed: int = 0) -> dict:
    key_list = jax.random.split(jax.random.key(seed), 5)
    tokens = bell_draw(key_list[0], (TOKENS, D), 1.0, 6.0, ((0, 16), (1, 8)))
    norm_gain = jnp.clip(1.0 + 0.18 * jax.random.normal(key_list[1], (D,), jnp.float32), 0.1, 1.9)
    up_master = bell_draw(key_list[2], (D, FF), D ** -0.5, 0.125, ((0, 16), (1, 8)), jnp.float32)
    down_master = bell_draw(key_list[3], (D, FF), FF ** -0.5, 0.0625, ((0, 16), (1, 8)), jnp.float32)
    return {"tokens": tokens, "norm_gain": norm_gain, "up_master": up_master, "down_master": down_master}


norm_floor = 1e-06

def reference(tokens, norm_gain, up_master, down_master):
    up_weights = (norm_gain[:, None] * up_master).astype(jnp.bfloat16)
    down_weights = jnp.transpose(down_master).astype(jnp.bfloat16)
    widened = tokens.astype(jnp.float32)
    normed = (widened * lax.rsqrt(lax.optimization_barrier(jnp.mean(widened * widened, axis=-1, keepdims=True)) + norm_floor)).astype(jnp.bfloat16)
    preact = jnp.dot(normed, up_weights, preferred_element_type=jnp.float32)
    hidden = jnp.square(jax.nn.relu(preact)).astype(jnp.bfloat16)
    block = FF // N_TP
    hidden_blocks = jnp.transpose(hidden.reshape(hidden.shape[0], N_TP, block), (1, 0, 2))
    down_blocks = down_weights.reshape(N_TP, block, D)

    def accumulate(total, pieces):
        partial_value = jnp.dot(pieces[0], pieces[1], preferred_element_type=jnp.float32).astype(jnp.bfloat16)
        partial_value = lax.optimization_barrier(partial_value)
        return (total + partial_value.astype(jnp.float32), None)
    start_total = jnp.zeros((hidden.shape[0], D), jnp.float32)
    total, unused = lax.scan(accumulate, start_total, (hidden_blocks, down_blocks))
    return (up_weights, down_weights, total.astype(jnp.bfloat16))
```

```python
import jax
import jax.numpy as jnp
from jax import lax
from jax.experimental import pallas as pl
from jax.experimental.pallas import tpu as pltpu
from jax.sharding import PartitionSpec as P

norm_floor = 1e-06

MESH = pl.DeviceIdType.MESH
BF, F32 = jnp.bfloat16, jnp.float32
D, FF = 2048, 8192
ROWS = 1024
TILE = 256
UP, DN = 0, 1


def kernel(
    tok_in, gain_in, up_in, dn_in,
    up_v, dn_v, out_v,
    up32, dn32, gain_v, tok_v, scale_v, hid, pbuf, prx, fwd, qf, fin,
    in_sem, w_send, w_recv, t_send, t_recv, r_send, r_recv,
):
    fs, tp = lax.axis_index("fs"), lax.axis_index("tp")
    z, y, x, c = fs // 4, fs % 4, tp // 2, tp % 2
    mod4 = lambda v: lax.rem(v + 8, 4)
    to_y = lambda s: {"fs": z * 4 + mod4(y + s), "tp": tp}
    to_z = lambda s: {"fs": mod4(z + s) * 4 + y, "tp": tp}
    to_x = lambda s: {"fs": fs, "tp": mod4(x + s) * 2 + c}
    partner = {"fs": fs, "tp": x * 2 + 1 - c}

    loads = [
        pltpu.make_async_copy(up_in, up32, in_sem.at[0]),
        pltpu.make_async_copy(gain_in, gain_v, in_sem.at[1]),
        pltpu.make_async_copy(tok_in, tok_v.at[tp], in_sem.at[2]),
        pltpu.make_async_copy(dn_in, dn32, in_sem.at[3]),
    ]
    for load in loads:
        load.start()
    barrier = pltpu.get_barrier_semaphore()
    for peer in (to_y(1), to_y(-1), to_z(1), to_z(-1), to_x(1), to_x(-1), partner):
        pl.semaphore_signal(barrier, inc=1, device_id=peer, device_id_type=MESH)

    sends = []

    def remote(src, dst, landed, send_sem, recv_sem, peer):
        out = lambda: pltpu.make_async_remote_copy(src, dst, send_sem, recv_sem, peer, MESH)
        back = lambda: pltpu.make_async_remote_copy(landed, landed, send_sem, recv_sem, peer, MESH)
        return out, back

    def go(pair):
        copy = pair[0]()
        copy.start()
        sends.append(copy)

    def weight_copies(w, h):
        first, second = (to_y, to_z) if h == 0 else (to_z, to_y)
        ia, ib = (y, z) if h == 0 else (z, y)

        def piece(da, db, q):
            a, b = mod4(ia + da), mod4(ib + db)
            f = b * 4 + a if h == 0 else a * 4 + b
            if w == UP:
                at, n = f * 128 + (0 if q is None else 64 * q), 128 if q is None else 64
                return up_v.at[h, pl.ds(pl.multiple_of(at, 64), n)]
            at, n = 512 * h + (0 if q is None else 256 * q), 512 if q is None else 256
            return dn_v.at[f, pl.ds(at, n)]

        table, count = {}, [0]

        def add(name, sent, peer, landed):
            k = count[0]
            count[0] += 1
            table[name] = remote(piece(*sent), piece(*sent), piece(*landed), w_send.at[w, h, k], w_recv.at[w, h, k], peer)

        for s, sign in (("+", 1), ("-", -1)):
            q = 0 if sign == 1 else 1
            add("S" + s, (0, 0, None), first(sign), (-sign, 0, None))
            add("F" + s, (-sign, 0, q), first(sign), (2, 0, q))
            for a in (0, -1, 1):
                add((a, "T" + s), (a, 0, None), second(sign), (a, -sign, None))
                add((a, "G" + s), (a, -sign, q), second(sign), (a, 2, q))
            for part in (0, 1):
                add((2, "T" + s, part), (2, 0, part), second(sign), (2, -sign, part))
            add((2, "G" + s), (2, -sign, q), second(sign), (2, 2, q))
        return table

    W = [[weight_copies(w, h) for h in (0, 1)] for w in (UP, DN)]

    def e0(w):
        for h in (0, 1):
            go(W[w][h]["S+"]), go(W[w][h]["S-"])
        for h in (0, 1):
            go(W[w][h][0, "T+"]), go(W[w][h][0, "T-"])

    def e1(w):
        for s, a in (("+", -1), ("-", 1)):
            for h in (0, 1):
                W[w][h]["S" + s][1]().wait_recv()
                go(W[w][h]["F" + s])
                go(W[w][h][a, "T+"]), go(W[w][h][a, "T-"])

    def e24(w, a):
        for s in ("+", "-"):
            for h in (0, 1):
                W[w][h][a, "T" + s][1]().wait_recv()
                go(W[w][h][a, "G" + s])

    def e3(w):
        for s, q in (("+", 0), ("-", 1)):
            for h in (0, 1):
                W[w][h]["F" + s][1]().wait_recv()
                go(W[w][h][2, "T+", q]), go(W[w][h][2, "T-", q])

    def e5(w):
        for s, q in (("+", 0), ("-", 1)):
            for h in (0, 1):
                W[w][h][2, "T" + s, q][1]().wait_recv()
                go(W[w][h][2, "G" + s])

    def landed(w, names):
        for h in (0, 1):
            for name in names:
                W[w][h][name][1]().wait_recv()

    own_far = [(0, "G+"), (0, "G-")]
    side_far = [(-1, "G+"), (-1, "G-"), (1, "G+"), (1, "G-"), (2, "T+", 1), (2, "T-", 0)]
    far_far = [(2, "G+"), (2, "G-")]

    def rows_of(t, half):
        return tok_v.at[t] if half is None else tok_v.at[t, pl.ds(512 * half, 512)]

    block = lambda d, core: mod4(x + d) * 2 + core
    T = {}

    def token_copy(name, d_sent, half, peer, d_landed, core_landed):
        k = len(T)
        sent, got = rows_of(block(d_sent, c), half), rows_of(block(d_landed, core_landed), half)
        T[name] = remote(sent, sent, got, t_send.at[k], t_recv.at[k], peer)

    for half in (0, 1):
        token_copy(("X+", half), 0, half, to_x(1), -1, c)
        token_copy(("X-", half), 0, half, to_x(-1), 1, c)
    token_copy("Y+", -1, 0, to_x(1), 2, c)
    token_copy("Y-", 1, 1, to_x(-1), 2, c)
    token_copy(("D", 0), 0, None, partner, 0, 1 - c)
    token_copy(("D", -1), -1, None, partner, -1, 1 - c)
    token_copy(("D", 1), 1, None, partner, 1, 1 - c)
    token_copy(("D", 2, 0), 2, 0, partner, 2, 1 - c)
    token_copy(("D", 2, 1), 2, 1, partner, 2, 1 - c)

    loads[0].wait()
    loads[1].wait()
    gain = jnp.transpose(jnp.broadcast_to(gain_v[...], (128, 128)))
    for h in (0, 1):
        for k in range(4):
            cols = slice(512 * h + 128 * k, 512 * h + 128 * k + 128)
            up_v[h, pl.ds(pl.multiple_of(fs * 128, 128), 128), 128 * k : 128 * k + 128] = (gain * up32[:, cols]).astype(BF)
    loads[2].wait()
    pl.semaphore_wait(barrier, 7)

    e0(UP)
    go(T["X+", 0]), go(T["X-", 1]), go(T["X+", 1]), go(T["X-", 0])
    go(T["D", 0])

    loads[3].wait()
    for k in range(8):
        dn_v[fs, 128 * k : 128 * k + 128, :] = jnp.transpose(dn32[:, 128 * k : 128 * k + 128]).astype(BF)

    e1(UP)
    T["X+", 0][1]().wait_recv()
    go(T["Y+"])
    T["X-", 1][1]().wait_recv()
    go(T["Y-"])
    e24(UP, 0)
    e3(UP)
    T["X+", 1][1]().wait_recv()
    go(T["D", -1])
    T["X-", 0][1]().wait_recv()
    go(T["D", 1])
    e24(UP, -1)
    e24(UP, 1)
    e5(UP)
    e0(DN)
    T["Y+"][1]().wait_recv()
    go(T["D", 2, 0])
    T["Y-"][1]().wait_recv()
    go(T["D", 2, 1])
    for name in (("D", 0), ("D", -1), ("D", 1), ("D", 2, 0), ("D", 2, 1)):
        T[name][1]().wait_recv()

    def factor(m, carry):
        rows = pl.ds(pl.multiple_of(m * 128, 128), 128)
        total = jnp.zeros((128, 128), F32)
        for t in range(8):
            v = tok_v[t, rows, :].astype(F32)
            total += v[:, :128] * v[:, :128] + v[:, 128:] * v[:, 128:]
        mean = jnp.sum(total, axis=1, keepdims=True) * (1.0 / D)
        scale_v[rows, :] = jnp.broadcast_to(lax.rsqrt(mean + norm_floor), (128, 128))
        return carry

    lax.fori_loop(0, ROWS // 128, factor, 0)

    def hidden_half(h):
        def tile(m, carry):
            rows = pl.ds(pl.multiple_of(m * TILE, TILE), TILE)
            total = jnp.zeros((TILE, 512), F32)
            for t in range(8):
                total += jnp.dot(tok_v[t, rows, :], up_v[h, 256 * t : 256 * t + 256, :], preferred_element_type=F32)
            factor_of = scale_v[rows, :]
            for k in range(4):
                v = jnp.maximum(total[:, 128 * k : 128 * k + 128] * factor_of, 0.0)
                hid[rows, 512 * h + 128 * k : 512 * h + 128 * k + 128] = (v * v).astype(BF)
            return carry

        lax.fori_loop(0, ROWS // TILE, tile, 0)

    landed(UP, own_far + side_far + far_far)
    hidden_half(0)
    e1(DN)
    hidden_half(1)
    e24(DN, 0)

    near = y // 2

    def remote_partial(dz, o):
        slot = pbuf.at[o, dz]
        return remote(slot, prx.at[dz], prx.at[dz], r_send.at[dz], r_recv.at[dz], partner)

    def core_of(o):
        return near if o == 0 else 1 - near

    def product(dz, o):
        t = mod4(z + dz) * 2 + core_of(o)

        def tile(m, carry):
            rows = pl.ds(pl.multiple_of(m * TILE, TILE), TILE)
            pair = jnp.concatenate([dn_v[2 * t], dn_v[2 * t + 1]], axis=1)
            pbuf[o, dz, rows, :] = jnp.dot(hid[rows, :], pair, preferred_element_type=F32).astype(BF)
            return carry

        lax.fori_loop(0, ROWS // TILE, tile, 0)

        @pl.when(core_of(o) != c)
        def _():
            remote_partial(dz, o)[0]().start()

    half_rows = lambda ref, q: ref.at[pl.ds(512 * q, 512)]
    def ring(sign):
        q, k = (0, 4) if sign == 1 else (1, 7)
        side = 0 if sign == 1 else 1
        first = lambda src: remote(half_rows(src, q), fwd.at[side], fwd.at[side], r_send.at[k], r_recv.at[k], to_x(sign))
        second = remote(qf.at[side], half_rows(fin.at[side], q), half_rows(fin.at[side], q), r_send.at[k + 1], r_recv.at[k + 1], to_x(sign))
        direct = lambda src: remote(half_rows(src, 1 - q), half_rows(fin.at[side], 1 - q), half_rows(fin.at[side], 1 - q), r_send.at[k + 2], r_recv.at[k + 2], to_x(sign))
        return first, second, direct

    RING = {1: ring(1), -1: ring(-1)}
    ahead = lambda dz: mod4(z + dz - x)

    def reduce_pair(dz, o):
        @pl.when(core_of(o) == c)
        def _():
            remote_partial(dz, o)[1]().wait_recv()

            def tile(m, carry):
                rows = pl.ds(pl.multiple_of(m * TILE, TILE), TILE)
                pbuf[o, dz, rows, :] = (pbuf[o, dz, rows, :].astype(F32) + prx[dz, rows, :].astype(F32)).astype(BF)
                return carry

            lax.fori_loop(0, ROWS // TILE, tile, 0)

            @pl.when(ahead(dz) == 2)
            def _():
                RING[1][0](pbuf.at[o, dz])[0]().start()
                RING[-1][0](pbuf.at[o, dz])[0]().start()

            for sign, d in ((1, 1), (-1, 3)):
                @pl.when(ahead(dz) == d)
                def _():
                    RING[sign][2](pbuf.at[o, dz])[0]().start()

    def forward(dz, o):
        @pl.when(core_of(o) == c)
        def _():
            for sign, d in ((1, 1), (-1, 3)):
                side, q = (0, 0) if sign == 1 else (1, 1)

                @pl.when(ahead(dz) == d)
                def _():
                    RING[sign][0](pbuf.at[o, dz])[1]().wait_recv()

                    def tile(m, carry):
                        at = m * TILE
                        here = pl.ds(pl.multiple_of(at, TILE), TILE)
                        mine = pl.ds(pl.multiple_of(512 * q + at, TILE), TILE)
                        qf[side, here, :] = (pbuf[o, dz, mine, :].astype(F32) + fwd[side, here, :].astype(F32)).astype(BF)
                        return carry

                    lax.fori_loop(0, 512 // TILE, tile, 0)
                    RING[sign][1][0]().start()

    product(0, 0)
    e3(DN)
    reduce_pair(0, 0)
    e24(DN, -1)
    e24(DN, 1)
    product(1, 0)
    product(3, 0)
    reduce_pair(1, 0)
    forward(0, 0)
    reduce_pair(3, 0)
    e5(DN)
    landed(DN, own_far)
    product(0, 1)
    forward(1, 0)
    reduce_pair(0, 1)
    forward(3, 0)
    landed(DN, side_far)
    product(2, 0)
    product(1, 1)
    reduce_pair(2, 0)
    product(3, 1)
    forward(0, 1)
    reduce_pair(1, 1)
    landed(DN, far_far)
    product(2, 1)
    reduce_pair(3, 1)
    forward(2, 0)
    forward(1, 1)
    reduce_pair(2, 1)
    forward(3, 1)
    forward(2, 1)

    mine = mod4(x - z)
    o_mine = jnp.where(near == c, 0, 1)
    for sign in (1, -1):
        RING[sign][1][1]().wait_recv()
        RING[sign][2](pbuf.at[0, 0])[1]().wait_recv()

    def last(m, carry):
        rows = pl.ds(pl.multiple_of(m * TILE, TILE), TILE)
        total = pbuf[o_mine, mine, rows, :].astype(F32) + fin[0, rows, :].astype(F32) + fin[1, rows, :].astype(F32)
        out_v[rows, :] = total.astype(BF)
        return carry

    lax.fori_loop(0, ROWS // TILE, last, 0)

    for send in sends:
        send.wait_send()
    for dz in range(4):
        remote_partial(dz, 0)[0]().wait_send()
    for sign in (1, -1):
        RING[sign][0](pbuf.at[0, 0])[0]().wait_send()
        RING[sign][1][0]().wait_send()
        RING[sign][2](pbuf.at[0, 0])[0]().wait_send()


def put_out(up_v, dn_v, out_v, up_out, dn_out, out, sem):
    copies = [pltpu.make_async_copy(out_v, out, sem.at[18])]
    for h in (0, 1):
        copies.append(pltpu.make_async_copy(up_v.at[h], up_out.at[:, pl.ds(512 * h, 512)], sem.at[h]))
    for f in range(16):
        copies.append(pltpu.make_async_copy(dn_v.at[f], dn_out.at[:, pl.ds(128 * f, 128)], sem.at[2 + f]))
    for copy in copies:
        copy.start()
    for copy in copies:
        copy.wait()


def on_device(tokens, norm_gain, up_master, down_master):
    anywhere, vmem = pl.BlockSpec(memory_space=pl.ANY), pl.BlockSpec(memory_space=pltpu.VMEM)
    in_hbm = lambda v: pltpu.with_memory_space_constraint(v, pltpu.HBM)
    held = pl.pallas_call(
        kernel,
        name="gather_mlp",
        out_shape=(
            pltpu.VMEM((2, D, 512), BF),
            pltpu.VMEM((16, 1024, 128), BF),
            pltpu.VMEM((ROWS, 256), BF),
        ),
        in_specs=[anywhere] * 4,
        out_specs=(vmem, vmem, vmem),
        scratch_shapes=[
            pltpu.VMEM((128, 1024), F32),
            pltpu.VMEM((128, 1024), F32),
            pltpu.VMEM((1, 128), F32),
            pltpu.VMEM((8, ROWS, 256), BF),
            pltpu.VMEM((ROWS, 128), F32),
            pltpu.VMEM((ROWS, 1024), BF),
            pltpu.VMEM((2, 4, ROWS, 256), BF),
            pltpu.VMEM((4, ROWS, 256), BF),
            pltpu.VMEM((2, 512, 256), BF),
            pltpu.VMEM((2, 512, 256), BF),
            pltpu.VMEM((2, ROWS, 256), BF),
            pltpu.SemaphoreType.DMA((4,)),
            pltpu.SemaphoreType.DMA((2, 2, 22)),
            pltpu.SemaphoreType.DMA((2, 2, 22)),
            pltpu.SemaphoreType.DMA((11,)),
            pltpu.SemaphoreType.DMA((11,)),
            pltpu.SemaphoreType.DMA((10,)),
            pltpu.SemaphoreType.DMA((10,)),
        ],
        compiler_params=pltpu.CompilerParams(collective_id=0, has_side_effects=True, vmem_limit_bytes=40 << 20),
    )(in_hbm(tokens), in_hbm(norm_gain.reshape(1, 128)), in_hbm(up_master), in_hbm(down_master))
    return pl.pallas_call(
        put_out,
        name="put_out",
        out_shape=(
            jax.ShapeDtypeStruct((D, 1024), BF),
            jax.ShapeDtypeStruct((1024, D), BF),
            jax.ShapeDtypeStruct((ROWS, 256), BF),
        ),
        in_specs=[vmem] * 3,
        out_specs=(anywhere,) * 3,
        scratch_shapes=[pltpu.SemaphoreType.DMA((19,))],
        compiler_params=pltpu.CompilerParams(vmem_limit_bytes=16 << 20),
    )(*held)


def solution(mesh):
    in_specs = (P("fs", "tp"), P("fs"), P("fs", "tp"), P("fs", "tp"))
    out_specs = (P(None, "tp"), P("tp", None), P("fs", "tp"))
    return jax.shard_map(
        on_device, mesh=mesh, in_specs=in_specs, out_specs=out_specs, check_vma=False
    )
```

```python
import jax
import jax.numpy as jnp
from jax import lax
from jax.experimental import pallas as pl
from jax.experimental.pallas import tpu as pltpu
from jax.sharding import PartitionSpec as P

norm_floor = 1e-06

MESH = pl.DeviceIdType.MESH
BF, F32 = jnp.bfloat16, jnp.float32
D, FF = 2048, 8192
ROWS = 1024
TILE = 512
UP, DN = 0, 1


def kernel(
    tok_in, gain_in, up_in, dn_in,
    up_v, dn_v, out_v,
    up32, dn32, gain_v, tok_v, scale_v, acc, hid, pbuf, prx, fwd, qf, fin,
    in_sem, w_send, w_recv, t_send, t_recv, p_send, p_recv, r_send, r_recv,
):
    fs, tp = lax.axis_index("fs"), lax.axis_index("tp")
    z, y, x, c = fs // 4, fs % 4, tp // 2, tp % 2
    mod4 = lambda v: lax.rem(v + 8, 4)
    to_y = lambda s: {"fs": z * 4 + mod4(y + s), "tp": tp}
    to_z = lambda s: {"fs": mod4(z + s) * 4 + y, "tp": tp}
    to_x = lambda s: {"fs": fs, "tp": mod4(x + s) * 2 + c}
    partner = {"fs": fs, "tp": x * 2 + 1 - c}

    loads = [
        pltpu.make_async_copy(up_in, up32, in_sem.at[0]),
        pltpu.make_async_copy(gain_in, gain_v, in_sem.at[1]),
        pltpu.make_async_copy(tok_in, tok_v.at[tp], in_sem.at[2]),
        pltpu.make_async_copy(dn_in, dn32, in_sem.at[3]),
    ]
    for load in loads:
        load.start()
    barrier = pltpu.get_barrier_semaphore()
    for peer in (to_y(1), to_y(-1), to_z(1), to_z(-1), to_x(1), to_x(-1), partner):
        pl.semaphore_signal(barrier, inc=1, device_id=peer, device_id_type=MESH)

    sends = []

    def remote(src, dst, landed, send_sem, recv_sem, peer):
        out = lambda: pltpu.make_async_remote_copy(src, dst, send_sem, recv_sem, peer, MESH)
        back = lambda: pltpu.make_async_remote_copy(landed, landed, send_sem, recv_sem, peer, MESH)
        return out, back

    def go(pair):
        copy = pair[0]()
        copy.start()
        sends.append(copy)

    toward = 1 - 2 * (y % 2)
    y_at = {0: 0, "+": toward, "-": -toward, 2: 2}

    def weight_copies(w):
        def piece(h, jy, jz, q):
            f = mod4(z + jz) * 4 + mod4(y + y_at[jy])
            if w == UP:
                at, n = f * 128 + (0 if q is None else 64 * q), 128 if q is None else 64
                return up_v.at[h, pl.ds(pl.multiple_of(at, 64), n)]
            at, n = 512 * h + (0 if q is None else 256 * q), 512 if q is None else 256
            return dn_v.at[f, pl.ds(at, n)]

        tables = ({}, {})

        def add(h, name, sent, side, landed):
            k = len(tables[h])
            peer = to_y(y_at[side]) if side in ("+", "-") else to_z(side)
            src, got = piece(h, *sent), piece(h, *landed)
            tables[h][name] = remote(src, src, got, w_send.at[w, h, k], w_recv.at[w, h, k], peer)

        for s, other, q in (("+", "-", 1), ("-", "+", 0)):
            add(0, ("S", s), (0, 0, None), s, (s, 0, None))
            add(0, ("F", s), (other, 0, q), s, (2, 0, q))
            for jz in (0, 1, -1):
                add(1, (jz, "T", s), (0, jz, None), s, (s, jz, None))
                add(1, (jz, "G", s), (other, jz, q), s, (2, jz, q))
            for part in (0, 1):
                add(1, (2, "T", s, part), (0, 2, part), s, (s, 2, part))
            add(1, (2, "G", s), (other, 2, q), s, (2, 2, q))
        for s, q in ((1, 0), (-1, 1)):
            add(1, ("S", s), (0, 0, None), s, (0, -s, None))
            add(1, ("F", s), (0, -s, q), s, (0, 2, q))
            for jy in (0, "+", "-"):
                add(0, (jy, "T", s), (jy, 0, None), s, (jy, -s, None))
                add(0, (jy, "G", s), (jy, -s, q), s, (jy, 2, q))
            for part in (0, 1):
                add(0, (2, "T", s, part), (2, 0, part), s, (2, -s, part))
            add(0, (2, "G", s), (2, -s, q), s, (2, 2, q))
        return tables

    W = [weight_copies(w) for w in (UP, DN)]

    def take(w, h, *names):
        for name in names:
            W[w][h][name][1]().wait_recv()

    def put(w, h, *names):
        for name in names:
            go(W[w][h][name])

    def e0y(w):
        put(w, 0, ("S", "+"), ("S", "-"))
        put(w, 1, (0, "T", "+"), (0, "T", "-"))

    def e0z(w):
        put(w, 1, ("S", 1), ("S", -1))
        put(w, 0, (0, "T", 1), (0, "T", -1))

    def e1(w):
        take(w, 0, ("S", "+"))
        put(w, 0, ("+", "T", 1), ("+", "T", -1), ("F", "-"))
        for s in (1, -1):
            take(w, 1, ("S", s))
            put(w, 1, (-s, "T", "+"), (-s, "T", "-"), ("F", s))
        take(w, 0, ("S", "-"))
        put(w, 0, ("F", "+"))

    def e2(w):
        for s in (1, -1):
            take(w, 0, (0, "T", s))
            put(w, 0, (0, "G", s))
        take(w, 1, (0, "T", "+"))
        put(w, 1, (0, "G", "-"))
        take(w, 1, (0, "T", "-"))

    def e3a(w):
        for s in (1, -1):
            take(w, 0, ("+", "T", s))
            put(w, 0, ("+", "G", s))

    def e3b(w):
        for s, q in ((1, 0), (-1, 1)):
            take(w, 1, ("F", s))
            put(w, 1, (2, "T", "+", q), (2, "T", "-", q))
        put(w, 0, ("-", "T", 1), ("-", "T", -1))
        put(w, 1, (0, "G", "+"))

    def e3c(w):
        for s, q in (("-", 0), ("+", 1)):
            take(w, 0, ("F", s))
            put(w, 0, (2, "T", 1, q), (2, "T", -1, q))

    def e4a(w):
        for jz in (-1, 1):
            for s, other in (("+", "-"), ("-", "+")):
                take(w, 1, (jz, "T", s))
                put(w, 1, (jz, "G", other))

    def own_far(w):
        take(w, 0, (0, "G", 1), (0, "G", -1), ("+", "G", 1), ("+", "G", -1))
        take(w, 1, (2, "T", "+", 0))
        put(w, 1, (2, "G", "-"))
        take(w, 1, (2, "T", "+", 1))

    def e4b(w):
        take(w, 1, (2, "T", "-", 1))
        put(w, 1, (2, "G", "+"))

    def e4c(w):
        for s in (1, -1):
            take(w, 0, ("-", "T", s))
            put(w, 0, ("-", "G", s))

    def e4d(w):
        for s, q in ((1, 0), (-1, 1)):
            take(w, 0, (2, "T", s, q))
            put(w, 0, (2, "G", s))

    def other_near(w):
        take(w, 1, (0, "G", "+"), (0, "G", "-"))

    def other_side(w):
        take(w, 0, (2, "T", 1, 1), (2, "T", -1, 0))
        take(w, 1, *[(jz, "G", s) for jz in (1, -1) for s in ("+", "-")])

    def other_far(w):
        take(w, 0, ("-", "G", 1), ("-", "G", -1), (2, "G", 1), (2, "G", -1))
        take(w, 1, (2, "T", "-", 0), (2, "G", "+"), (2, "G", "-"))

    def rows_of(t, half):
        return tok_v.at[t] if half is None else tok_v.at[t, pl.ds(512 * half, 512)]

    block = lambda d, core: mod4(x + d) * 2 + core
    T = {}

    def token_copy(name, d_sent, half, peer, d_landed, core_landed):
        k = len(T)
        sent, got = rows_of(block(d_sent, c), half), rows_of(block(d_landed, core_landed), half)
        T[name] = remote(sent, sent, got, t_send.at[k], t_recv.at[k], peer)

    for half in (0, 1):
        token_copy(("X+", half), 0, half, to_x(1), -1, c)
        token_copy(("X-", half), 0, half, to_x(-1), 1, c)
    token_copy("Y+", -1, 0, to_x(1), 2, c)
    token_copy("Y-", 1, 1, to_x(-1), 2, c)
    token_copy(("D", 0), 0, None, partner, 0, 1 - c)
    token_copy(("D", -1), -1, None, partner, -1, 1 - c)
    token_copy(("D", 1), 1, None, partner, 1, 1 - c)
    token_copy(("D", 2, 0), 2, 0, partner, 2, 1 - c)
    token_copy(("D", 2, 1), 2, 1, partner, 2, 1 - c)

    loads[0].wait()
    loads[1].wait()
    gain = jnp.transpose(jnp.broadcast_to(gain_v[...], (128, 128)))
    for h in (0, 1):
        for k in range(4):
            cols = slice(512 * h + 128 * k, 512 * h + 128 * k + 128)
            up_v[h, pl.ds(pl.multiple_of(fs * 128, 128), 128), 128 * k : 128 * k + 128] = (gain * up32[:, cols]).astype(BF)
    loads[2].wait()
    pl.semaphore_wait(barrier, 7)

    e0y(UP)
    e0z(UP)
    go(T["X+", 0]), go(T["X-", 1]), go(T["X+", 1]), go(T["X-", 0])
    go(T["D", 0])

    loads[3].wait()
    for k in range(8):
        dn_v[fs, 128 * k : 128 * k + 128, :] = jnp.transpose(dn32[:, 128 * k : 128 * k + 128]).astype(BF)

    e1(UP)
    e2(UP)
    T["X+", 0][1]().wait_recv()
    go(T["Y+"])
    T["X-", 1][1]().wait_recv()
    go(T["Y-"])
    e3a(UP)
    e3b(UP)
    e4a(UP)
    T["X+", 1][1]().wait_recv()
    go(T["D", -1])
    T["X-", 0][1]().wait_recv()
    go(T["D", 1])
    e3c(UP)
    e4c(UP)
    own_far(UP)
    e4b(UP)
    e0y(DN)
    T["Y+"][1]().wait_recv()
    go(T["D", 2, 0])
    T["Y-"][1]().wait_recv()
    go(T["D", 2, 1])
    e4d(UP)
    e0z(DN)
    for name in (("D", 0), ("D", -1), ("D", 1), ("D", 2, 0), ("D", 2, 1)):
        T[name][1]().wait_recv()

    def factor(m, carry):
        rows = pl.ds(pl.multiple_of(m * 128, 128), 128)
        total = jnp.zeros((128, 128), F32)
        for t in range(8):
            v = tok_v[t, rows, :].astype(F32)
            total += v[:, :128] * v[:, :128] + v[:, 128:] * v[:, 128:]
        mean = jnp.sum(total, axis=1, keepdims=True) * (1.0 / D)
        scale_v[rows, :] = jnp.broadcast_to(lax.rsqrt(mean + norm_floor), (128, 128))
        return carry

    lax.fori_loop(0, ROWS // 128, factor, 0)

    near = y // 2

    def core_of(o):
        return near if o == 0 else 1 - near

    def pair_of(dz, o):
        return mod4(z + dz) * 2 + core_of(o)

    def dots(h, rows, pairs):
        total = None
        for pair in pairs:
            t = pair_of(*pair)
            weights = up_v[h, pl.ds(pl.multiple_of(256 * t, 256), 256), :]
            term = jnp.dot(tok_v[t, rows, :], weights, preferred_element_type=F32)
            total = term if total is None else total + term
        return total

    def first_part(i, carry):
        h, m = i // (ROWS // TILE), lax.rem(i, ROWS // TILE)
        rows = pl.ds(pl.multiple_of(m * TILE, TILE), TILE)
        acc[h, rows, :] = dots(h, rows, ((0, 0), (1, 0), (3, 0), (2, 0)))
        return carry

    def second_part(h):
        def tile(m, carry):
            rows = pl.ds(pl.multiple_of(m * TILE, TILE), TILE)
            total = acc[h, rows, :] + dots(h, rows, ((0, 1), (1, 1), (3, 1), (2, 1)))
            factor_of = scale_v[rows, :]
            for k in range(4):
                v = jnp.maximum(total[:, 128 * k : 128 * k + 128] * factor_of, 0.0)
                hid[rows, 512 * h + 128 * k : 512 * h + 128 * k + 128] = (v * v).astype(BF)
            return carry

        lax.fori_loop(0, ROWS // TILE, tile, 0)

    lax.fori_loop(0, 2 * ROWS // TILE, first_part, 0)
    other_near(UP)
    other_side(UP)
    other_far(UP)
    second_part(0)
    e1(DN)
    second_part(1)
    e2(DN)

    def remote_partial(dz, o, r):
        part = pl.ds(pl.multiple_of(512 * r, 512), 512)
        return remote(pbuf.at[o, dz, part], prx.at[dz, part], prx.at[dz, part], p_send.at[dz, r], p_recv.at[dz, r], partner)

    def product(dz, o):
        t = pair_of(dz, o)

        def tile(r, carry):
            rows = pl.ds(pl.multiple_of(r * 512, 512), 512)
            pair = jnp.concatenate([dn_v[2 * t], dn_v[2 * t + 1]], axis=1)
            pbuf[o, dz, rows, :] = jnp.dot(hid[rows, :], pair, preferred_element_type=F32).astype(BF)

            @pl.when(core_of(o) != c)
            def _():
                remote_partial(dz, o, r)[0]().start()

            return carry

        lax.fori_loop(0, 2, tile, 0)

    def ring(sign):
        side = 0 if sign == 1 else 1
        q, k, peer = side, 5 * side, to_x(sign)
        chunk = lambda ref, base, j: ref.at[pl.ds(base + 256 * j, 256)]

        def first(src, j):
            got = chunk(fwd.at[side], 0, j)
            return remote(chunk(src, 512 * q, j), got, got, r_send.at[k + j], r_recv.at[k + j], peer)

        def second(j):
            got = chunk(fin.at[side], 512 * q, j)
            return remote(chunk(qf.at[side], 0, j), got, got, r_send.at[k + 2 + j], r_recv.at[k + 2 + j], peer)

        def direct(src):
            rows = pl.ds(512 * (1 - q), 512)
            return remote(src.at[rows], fin.at[side, rows], fin.at[side, rows], r_send.at[k + 4], r_recv.at[k + 4], peer)

        return first, second, direct

    RING = {1: ring(1), -1: ring(-1)}
    ahead = lambda dz: mod4(z + dz - x)

    def reduce_pair(dz, o):
        @pl.when(core_of(o) == c)
        def _():
            mine = pbuf.at[o, dz]
            for r, sign, d in ((0, 1, 3), (1, -1, 1)):
                remote_partial(dz, o, r)[1]().wait_recv()
                rows = pl.ds(512 * r, 512)
                pbuf[o, dz, rows, :] = (pbuf[o, dz, rows, :].astype(F32) + prx[dz, rows, :].astype(F32)).astype(BF)

                @pl.when(ahead(dz) == 2)
                def _():
                    RING[sign][0](mine, 0)[0]().start()
                    RING[sign][0](mine, 1)[0]().start()

                @pl.when(ahead(dz) == d)
                def _():
                    RING[-sign][2](mine)[0]().start()

    def forward(dz, o):
        @pl.when(core_of(o) == c)
        def _():
            for sign, d in ((1, 1), (-1, 3)):
                side = 0 if sign == 1 else 1

                @pl.when(ahead(dz) == d)
                def _():
                    for j in (0, 1):
                        RING[sign][0](pbuf.at[o, dz], j)[1]().wait_recv()
                        here, mine = pl.ds(256 * j, 256), pl.ds(512 * side + 256 * j, 256)
                        qf[side, here, :] = (pbuf[o, dz, mine, :].astype(F32) + fwd[side, here, :].astype(F32)).astype(BF)
                        RING[sign][1](j)[0]().start()

    product(0, 0)
    e3a(DN)
    reduce_pair(0, 0)
    e3b(DN)
    e4a(DN)
    product(1, 0)
    forward(0, 0)
    product(3, 0)
    e3c(DN)
    reduce_pair(1, 0)
    reduce_pair(3, 0)
    e4c(DN)
    own_far(DN)
    product(2, 0)
    e4b(DN)
    other_near(DN)
    product(0, 1)
    reduce_pair(2, 0)
    e4d(DN)
    other_side(DN)
    product(1, 1)
    reduce_pair(0, 1)
    product(3, 1)
    reduce_pair(1, 1)
    other_far(DN)
    product(2, 1)
    forward(3, 0)
    forward(1, 0)
    reduce_pair(3, 1)
    forward(2, 0)
    reduce_pair(2, 1)
    forward(0, 1)
    forward(1, 1)
    forward(3, 1)
    forward(2, 1)

    mine = mod4(x - z)
    o_mine = jnp.where(near == c, 0, 1)
    for sign in (1, -1):
        RING[sign][1](0)[1]().wait_recv()
        RING[sign][1](1)[1]().wait_recv()
        RING[sign][2](pbuf.at[0, 0])[1]().wait_recv()

    def last(m, carry):
        rows = pl.ds(pl.multiple_of(m * TILE, TILE), TILE)
        total = pbuf[o_mine, mine, rows, :].astype(F32) + fin[0, rows, :].astype(F32) + fin[1, rows, :].astype(F32)
        out_v[rows, :] = total.astype(BF)
        return carry

    lax.fori_loop(0, ROWS // TILE, last, 0)

    for send in sends:
        send.wait_send()
    for dz in range(4):
        for r in (0, 1):
            remote_partial(dz, 0, r)[0]().wait_send()
    for sign in (1, -1):
        for j in (0, 1):
            RING[sign][0](pbuf.at[0, 0], j)[0]().wait_send()
            RING[sign][1](j)[0]().wait_send()
        RING[sign][2](pbuf.at[0, 0])[0]().wait_send()


def put_out(up_v, dn_v, out_v, up_out, dn_out, out, sem):
    copies = [pltpu.make_async_copy(out_v, out, sem.at[18])]
    for h in (0, 1):
        copies.append(pltpu.make_async_copy(up_v.at[h], up_out.at[:, pl.ds(512 * h, 512)], sem.at[h]))
    for f in range(16):
        copies.append(pltpu.make_async_copy(dn_v.at[f], dn_out.at[:, pl.ds(128 * f, 128)], sem.at[2 + f]))
    for copy in copies:
        copy.start()
    for copy in copies:
        copy.wait()


def on_device(tokens, norm_gain, up_master, down_master):
    anywhere, vmem = pl.BlockSpec(memory_space=pl.ANY), pl.BlockSpec(memory_space=pltpu.VMEM)
    in_hbm = lambda v: pltpu.with_memory_space_constraint(v, pltpu.HBM)
    held = pl.pallas_call(
        kernel,
        name="gather_mlp",
        out_shape=(
            pltpu.VMEM((2, D, 512), BF),
            pltpu.VMEM((16, 1024, 128), BF),
            pltpu.VMEM((ROWS, 256), BF),
        ),
        in_specs=[anywhere] * 4,
        out_specs=(vmem, vmem, vmem),
        scratch_shapes=[
            pltpu.VMEM((128, 1024), F32),
            pltpu.VMEM((128, 1024), F32),
            pltpu.VMEM((1, 128), F32),
            pltpu.VMEM((8, ROWS, 256), BF),
            pltpu.VMEM((ROWS, 128), F32),
            pltpu.VMEM((2, ROWS, 512), F32),
            pltpu.VMEM((ROWS, 1024), BF),
            pltpu.VMEM((2, 4, ROWS, 256), BF),
            pltpu.VMEM((4, ROWS, 256), BF),
            pltpu.VMEM((2, 512, 256), BF),
            pltpu.VMEM((2, 512, 256), BF),
            pltpu.VMEM((2, ROWS, 256), BF),
            pltpu.SemaphoreType.DMA((4,)),
            pltpu.SemaphoreType.DMA((2, 2, 22)),
            pltpu.SemaphoreType.DMA((2, 2, 22)),
            pltpu.SemaphoreType.DMA((11,)),
            pltpu.SemaphoreType.DMA((11,)),
            pltpu.SemaphoreType.DMA((4, 2)),
            pltpu.SemaphoreType.DMA((4, 2)),
            pltpu.SemaphoreType.DMA((10,)),
            pltpu.SemaphoreType.DMA((10,)),
        ],
        compiler_params=pltpu.CompilerParams(collective_id=0, has_side_effects=True, vmem_limit_bytes=40 << 20),
    )(in_hbm(tokens), in_hbm(norm_gain.reshape(1, 128)), in_hbm(up_master), in_hbm(down_master))
    return pl.pallas_call(
        put_out,
        name="put_out",
        out_shape=(
            jax.ShapeDtypeStruct((D, 1024), BF),
            jax.ShapeDtypeStruct((1024, D), BF),
            jax.ShapeDtypeStruct((ROWS, 256), BF),
        ),
        in_specs=[vmem] * 3,
        out_specs=(anywhere,) * 3,
        scratch_shapes=[pltpu.SemaphoreType.DMA((19,))],
        compiler_params=pltpu.CompilerParams(vmem_limit_bytes=16 << 20),
    )(*held)


def solution(mesh):
    in_specs = (P("fs", "tp"), P("fs"), P("fs", "tp"), P("fs", "tp"))
    out_specs = (P(None, "tp"), P("tp", None), P("fs", "tp"))
    return jax.shard_map(
        on_device, mesh=mesh, in_specs=in_specs, out_specs=out_specs, check_vma=False
    )
```

```python
import jax
import jax.numpy as jnp
from jax import lax
from jax.experimental import pallas as pl
from jax.experimental.pallas import tpu as pltpu
from jax.sharding import PartitionSpec as P

norm_floor = 1e-06

MESH = pl.DeviceIdType.MESH
BF, F32 = jnp.bfloat16, jnp.float32
D, FF = 2048, 8192
ROWS = 1024
TILE = 512
UP, DN = 0, 1


def kernel(
    tok_in, gain_in, up_in, dn_in,
    up_v, dn_v, out_v,
    up32, dn32, gain_v, tok_v, scale_v, acc, hid, pbuf, prx, fwd, qf, fin,
    in_sem, sent_sem, w_recv, t_recv, p_recv, r_recv,
):
    fs, tp = lax.axis_index("fs"), lax.axis_index("tp")
    z, y, x, c = fs // 4, fs % 4, tp // 2, tp % 2
    mod4 = lambda v: lax.rem(v + 8, 4)
    to_y = lambda s: {"fs": z * 4 + mod4(y + s), "tp": tp}
    to_z = lambda s: {"fs": mod4(z + s) * 4 + y, "tp": tp}
    to_x = lambda s: {"fs": fs, "tp": mod4(x + s) * 2 + c}
    partner = {"fs": fs, "tp": x * 2 + 1 - c}

    loads = [
        pltpu.make_async_copy(up_in, up32, in_sem.at[0]),
        pltpu.make_async_copy(gain_in, gain_v, in_sem.at[1]),
        pltpu.make_async_copy(tok_in, tok_v.at[tp], in_sem.at[2]),
        pltpu.make_async_copy(dn_in, dn32, in_sem.at[3]),
    ]
    for load in loads:
        load.start()
    barrier = pltpu.get_barrier_semaphore()
    for peer in (to_y(1), to_y(-1), to_z(1), to_z(-1), to_x(1), to_x(-1), partner):
        pl.semaphore_signal(barrier, inc=1, device_id=peer, device_id_type=MESH)

    def remote(src, dst, landed, send_sem, recv_sem, peer):
        out = lambda: pltpu.make_async_remote_copy(src, dst, send_sem, recv_sem, peer, MESH)
        back = lambda: pltpu.make_async_remote_copy(landed, landed, send_sem, recv_sem, peer, MESH)
        return out, back

    def go(pair):
        pair[0]().start()

    toward = 1 - 2 * (y % 2)
    y_at = {0: 0, "+": toward, "-": -toward, 2: 2}

    def weight_copies(w):
        def piece(h, jy, jz, q):
            f = mod4(z + jz) * 4 + mod4(y + y_at[jy])
            if w == UP:
                at, n = f * 128 + (0 if q is None else 64 * q), 128 if q is None else 64
                return up_v.at[h, pl.ds(pl.multiple_of(at, 64), n)]
            at, n = 512 * h + (0 if q is None else 256 * q), 512 if q is None else 256
            return dn_v.at[f, pl.ds(at, n)]

        tables = ({}, {})

        def add(h, name, sent, side, landed):
            k = len(tables[h])
            peer = to_y(y_at[side]) if side in ("+", "-") else to_z(side)
            src, got = piece(h, *sent), piece(h, *landed)
            tables[h][name] = remote(src, src, got, sent_sem.at[w], w_recv.at[w, h, k], peer)

        for s, other, q in (("+", "-", 1), ("-", "+", 0)):
            add(0, ("S", s), (0, 0, None), s, (s, 0, None))
            add(0, ("F", s), (other, 0, q), s, (2, 0, q))
            for jz in (0, 1, -1):
                add(1, (jz, "T", s), (0, jz, None), s, (s, jz, None))
                add(1, (jz, "G", s), (other, jz, q), s, (2, jz, q))
            for part in (0, 1):
                add(1, (2, "T", s, part), (0, 2, part), s, (s, 2, part))
            add(1, (2, "G", s), (other, 2, q), s, (2, 2, q))
        for s, q in ((1, 0), (-1, 1)):
            add(1, ("S", s), (0, 0, None), s, (0, -s, None))
            add(1, ("F", s), (0, -s, q), s, (0, 2, q))
            for jy in (0, "+", "-"):
                add(0, (jy, "T", s), (jy, 0, None), s, (jy, -s, None))
                add(0, (jy, "G", s), (jy, -s, q), s, (jy, 2, q))
            for part in (0, 1):
                add(0, (2, "T", s, part), (2, 0, part), s, (2, -s, part))
            add(0, (2, "G", s), (2, -s, q), s, (2, 2, q))
        return tables

    W = [weight_copies(w) for w in (UP, DN)]

    def take(w, h, *names):
        for name in names:
            W[w][h][name][1]().wait_recv()

    def put(w, h, *names):
        for name in names:
            go(W[w][h][name])

    def e0y(w):
        put(w, 0, ("S", "+"), ("S", "-"))
        put(w, 1, (0, "T", "+"), (0, "T", "-"))

    def e0z(w):
        put(w, 1, ("S", 1), ("S", -1))
        put(w, 0, (0, "T", 1), (0, "T", -1))

    def e1(w):
        take(w, 0, ("S", "+"))
        put(w, 0, ("+", "T", 1), ("+", "T", -1), ("F", "-"))
        for s in (1, -1):
            take(w, 1, ("S", s))
            put(w, 1, (-s, "T", "+"), (-s, "T", "-"), ("F", s))
        take(w, 0, ("S", "-"))
        put(w, 0, ("F", "+"))

    def e2(w):
        for s in (1, -1):
            take(w, 0, (0, "T", s))
            put(w, 0, (0, "G", s))
        take(w, 1, (0, "T", "+"))
        put(w, 1, (0, "G", "-"))
        take(w, 1, (0, "T", "-"))

    def e3a(w):
        for s in (1, -1):
            take(w, 0, ("+", "T", s))
            put(w, 0, ("+", "G", s))

    def e3b(w):
        for s, q in ((1, 0), (-1, 1)):
            take(w, 1, ("F", s))
            put(w, 1, (2, "T", "+", q), (2, "T", "-", q))
        put(w, 0, ("-", "T", 1), ("-", "T", -1))
        put(w, 1, (0, "G", "+"))

    def e3c(w):
        for s, q in (("-", 0), ("+", 1)):
            take(w, 0, ("F", s))
            put(w, 0, (2, "T", 1, q), (2, "T", -1, q))

    def e4a(w):
        for jz in (-1, 1):
            for s, other in (("+", "-"), ("-", "+")):
                take(w, 1, (jz, "T", s))
                put(w, 1, (jz, "G", other))

    def own_far(w):
        take(w, 0, (0, "G", 1), (0, "G", -1), ("+", "G", 1), ("+", "G", -1))
        take(w, 1, (2, "T", "+", 0))
        put(w, 1, (2, "G", "-"))
        take(w, 1, (2, "T", "+", 1))

    def e4b(w):
        take(w, 1, (2, "T", "-", 1))
        put(w, 1, (2, "G", "+"))

    def e4c(w):
        for s in (1, -1):
            take(w, 0, ("-", "T", s))
            put(w, 0, ("-", "G", s))

    def e4d(w):
        for s, q in ((1, 0), (-1, 1)):
            take(w, 0, (2, "T", s, q))
            put(w, 0, (2, "G", s))

    def other_near(w):
        take(w, 1, (0, "G", "+"), (0, "G", "-"))

    def other_side(w):
        take(w, 0, (2, "T", 1, 1), (2, "T", -1, 0))
        take(w, 1, *[(jz, "G", s) for jz in (1, -1) for s in ("+", "-")])

    def other_far(w):
        take(w, 0, ("-", "G", 1), ("-", "G", -1), (2, "G", 1), (2, "G", -1))
        take(w, 1, (2, "T", "-", 0), (2, "G", "+"), (2, "G", "-"))

    def rows_of(t, half):
        return tok_v.at[t] if half is None else tok_v.at[t, pl.ds(512 * half, 512)]

    block = lambda d, core: mod4(x + d) * 2 + core
    T = {}

    def token_copy(name, d_sent, half, peer, d_landed, core_landed):
        k = len(T)
        sent, got = rows_of(block(d_sent, c), half), rows_of(block(d_landed, core_landed), half)
        T[name] = remote(sent, sent, got, sent_sem.at[2], t_recv.at[k], peer)

    for half in (0, 1):
        token_copy(("X+", half), 0, half, to_x(1), -1, c)
        token_copy(("X-", half), 0, half, to_x(-1), 1, c)
    token_copy("Y+", -1, 0, to_x(1), 2, c)
    token_copy("Y-", 1, 1, to_x(-1), 2, c)
    token_copy(("D", 0), 0, None, partner, 0, 1 - c)
    token_copy(("D", -1), -1, None, partner, -1, 1 - c)
    token_copy(("D", 1), 1, None, partner, 1, 1 - c)
    token_copy(("D", 2, 0), 2, 0, partner, 2, 1 - c)
    token_copy(("D", 2, 1), 2, 1, partner, 2, 1 - c)

    loads[0].wait()
    loads[1].wait()
    gain = jnp.transpose(jnp.broadcast_to(gain_v[...], (128, 128)))
    for h in (0, 1):
        for k in range(4):
            cols = slice(512 * h + 128 * k, 512 * h + 128 * k + 128)
            up_v[h, pl.ds(pl.multiple_of(fs * 128, 128), 128), 128 * k : 128 * k + 128] = (gain * up32[:, cols]).astype(BF)
    loads[2].wait()
    pl.semaphore_wait(barrier, 7)

    e0y(UP)
    e0z(UP)
    go(T["X+", 0]), go(T["X-", 1]), go(T["X+", 1]), go(T["X-", 0])
    go(T["D", 0])

    loads[3].wait()
    for k in range(8):
        dn_v[fs, 128 * k : 128 * k + 128, :] = jnp.transpose(dn32[:, 128 * k : 128 * k + 128]).astype(BF)

    e1(UP)
    e2(UP)
    T["X+", 0][1]().wait_recv()
    go(T["Y+"])
    T["X-", 1][1]().wait_recv()
    go(T["Y-"])
    e3a(UP)
    e3b(UP)
    T["X+", 1][1]().wait_recv()
    go(T["D", -1])
    T["X-", 0][1]().wait_recv()
    go(T["D", 1])
    e4a(UP)
    e3c(UP)
    e4c(UP)
    own_far(UP)
    T["Y+"][1]().wait_recv()
    go(T["D", 2, 0])
    T["Y-"][1]().wait_recv()
    go(T["D", 2, 1])
    e4b(UP)
    e0y(DN)
    e4d(UP)
    e0z(DN)
    for name in (("D", 0), ("D", -1), ("D", 1), ("D", 2, 0), ("D", 2, 1)):
        T[name][1]().wait_recv()

    ones = jnp.ones((128, 128), BF)

    def factor(m, carry):
        rows = pl.ds(pl.multiple_of(m * 256, 256), 256)
        total = jnp.zeros((256, 128), F32)
        for t in range(8):
            v = tok_v[t, rows, :].astype(F32)
            total += v[:, :128] * v[:, :128] + v[:, 128:] * v[:, 128:]
        high = total.astype(BF)
        low = (total - high.astype(F32)).astype(BF)
        summed = jnp.dot(high, ones, preferred_element_type=F32) + jnp.dot(low, ones, preferred_element_type=F32)
        scale_v[rows, :] = lax.rsqrt(summed * (1.0 / D) + norm_floor)
        return carry

    lax.fori_loop(0, ROWS // 256, factor, 0)

    near = y // 2

    def core_of(o):
        return near if o == 0 else 1 - near

    def pair_of(dz, o):
        return mod4(z + dz) * 2 + core_of(o)

    def dots(h, rows, pairs):
        total = None
        for pair in pairs:
            t = pair_of(*pair)
            weights = up_v[h, pl.ds(pl.multiple_of(256 * t, 256), 256), :]
            term = jnp.dot(tok_v[t, rows, :], weights, preferred_element_type=F32)
            total = term if total is None else total + term
        return total

    def first_part(i, carry):
        h, m = i // (ROWS // TILE), lax.rem(i, ROWS // TILE)
        rows = pl.ds(pl.multiple_of(m * TILE, TILE), TILE)
        acc[h, rows, :] = dots(h, rows, ((0, 0), (1, 0), (3, 0), (2, 0)))
        return carry

    def second_part(h):
        def tile(m, carry):
            rows = pl.ds(pl.multiple_of(m * TILE, TILE), TILE)
            total = acc[h, rows, :] + dots(h, rows, ((0, 1), (1, 1), (3, 1), (2, 1)))
            factor_of = scale_v[rows, :]
            for k in range(4):
                v = jnp.maximum(total[:, 128 * k : 128 * k + 128] * factor_of, 0.0)
                hid[rows, 512 * h + 128 * k : 512 * h + 128 * k + 128] = (v * v).astype(BF)
            return carry

        lax.fori_loop(0, ROWS // TILE, tile, 0)

    lax.fori_loop(0, 2 * ROWS // TILE, first_part, 0)
    other_near(UP)
    other_side(UP)
    other_far(UP)
    second_part(0)
    e1(DN)
    second_part(1)
    e2(DN)

    def remote_partial(dz, o, r):
        part = pl.ds(pl.multiple_of(512 * r, 512), 512)
        return remote(pbuf.at[o, dz, part], prx.at[dz, part], prx.at[dz, part], sent_sem.at[3], p_recv.at[dz, r], partner)

    def product(dz, o):
        t = pair_of(dz, o)

        def tile(r, carry):
            rows = pl.ds(pl.multiple_of(r * 512, 512), 512)
            pair = jnp.concatenate([dn_v[2 * t], dn_v[2 * t + 1]], axis=1)
            pbuf[o, dz, rows, :] = jnp.dot(hid[rows, :], pair, preferred_element_type=F32).astype(BF)

            @pl.when(core_of(o) != c)
            def _():
                remote_partial(dz, o, r)[0]().start()

            return carry

        lax.fori_loop(0, 2, tile, 0)

    def ring(sign):
        side = 0 if sign == 1 else 1
        q, k, peer = side, 6 * side, to_x(sign)
        chunk = lambda ref, base, j: ref.at[pl.ds(base + 256 * j, 256)]

        def first(src, j):
            got = chunk(fwd.at[side], 0, j)
            return remote(chunk(src, 512 * q, j), got, got, sent_sem.at[4], r_recv.at[k + j], peer)

        def second(j):
            got = chunk(fin.at[side], 512 * q, j)
            return remote(chunk(qf.at[side], 0, j), got, got, sent_sem.at[4], r_recv.at[k + 2 + j], peer)

        def direct(src, j):
            got = chunk(fin.at[side], 512 * (1 - q), j)
            return remote(chunk(src, 512 * (1 - q), j), got, got, sent_sem.at[4], r_recv.at[k + 4 + j], peer)

        return first, second, direct

    RING = {1: ring(1), -1: ring(-1)}
    ahead = lambda dz: mod4(z + dz - x)

    def reduce_pair(dz, o):
        @pl.when(core_of(o) == c)
        def _():
            mine = pbuf.at[o, dz]
            for r, sign, d in ((0, 1, 3), (1, -1, 1)):
                remote_partial(dz, o, r)[1]().wait_recv()
                rows = pl.ds(512 * r, 512)
                pbuf[o, dz, rows, :] = (pbuf[o, dz, rows, :].astype(F32) + prx[dz, rows, :].astype(F32)).astype(BF)

                @pl.when(ahead(dz) == 2)
                def _():
                    RING[sign][0](mine, 0)[0]().start()
                    RING[sign][0](mine, 1)[0]().start()

                @pl.when(ahead(dz) == d)
                def _():
                    RING[-sign][2](mine, 0)[0]().start()
                    if not later(dz, o):
                        RING[-sign][2](mine, 1)[0]().start()

    later = lambda dz, o: o == 1 and dz in (1, 3)

    def direct_rest(dz, o):
        @pl.when(core_of(o) == c)
        def _():
            for sign, d in ((1, 1), (-1, 3)):
                @pl.when(ahead(dz) == d)
                def _():
                    RING[sign][2](pbuf.at[o, dz], 1)[0]().start()

    def forward(dz, o):
        @pl.when(core_of(o) == c)
        def _():
            for sign, d in ((1, 1), (-1, 3)):
                side = 0 if sign == 1 else 1

                @pl.when(ahead(dz) == d)
                def _():
                    for j in (0, 1):
                        RING[sign][0](pbuf.at[o, dz], j)[1]().wait_recv()
                        here, mine = pl.ds(256 * j, 256), pl.ds(512 * side + 256 * j, 256)
                        qf[side, here, :] = (pbuf[o, dz, mine, :].astype(F32) + fwd[side, here, :].astype(F32)).astype(BF)
                        RING[sign][1](j)[0]().start()

    product(0, 0)
    e3a(DN)
    reduce_pair(0, 0)
    e3b(DN)
    e4a(DN)
    product(1, 0)
    e3c(DN)
    product(3, 0)
    reduce_pair(1, 0)
    reduce_pair(3, 0)
    forward(0, 0)
    e4c(DN)
    own_far(DN)
    product(2, 0)
    e4b(DN)
    other_near(DN)
    product(0, 1)
    reduce_pair(2, 0)
    e4d(DN)
    other_side(DN)
    product(1, 1)
    reduce_pair(0, 1)
    product(3, 1)
    forward(3, 0)
    reduce_pair(1, 1)
    forward(1, 0)
    reduce_pair(3, 1)
    other_far(DN)
    product(2, 1)
    forward(2, 0)
    reduce_pair(2, 1)
    direct_rest(1, 1)
    direct_rest(3, 1)
    forward(0, 1)
    forward(1, 1)
    forward(3, 1)
    forward(2, 1)

    mine = mod4(x - z)
    o_mine = jnp.where(near == c, 0, 1)
    for sign in (1, -1):
        RING[sign][1](0)[1]().wait_recv()
        RING[sign][1](1)[1]().wait_recv()
        RING[sign][2](pbuf.at[0, 0], 0)[1]().wait_recv()
        RING[sign][2](pbuf.at[0, 0], 1)[1]().wait_recv()

    def last(m, carry):
        rows = pl.ds(pl.multiple_of(m * TILE, TILE), TILE)
        total = pbuf[o_mine, mine, rows, :].astype(F32) + fin[0, rows, :].astype(F32) + fin[1, rows, :].astype(F32)
        out_v[rows, :] = total.astype(BF)
        return carry

    lax.fori_loop(0, ROWS // TILE, last, 0)

    for k, ref in enumerate((up_v.at[:, pl.ds(0, 1920)], dn_v.at[pl.ds(0, 15)], tok_v.at[pl.ds(0, 7)], prx, pbuf.at[0, pl.ds(0, 3)])):
        pltpu.make_async_copy(ref, ref, sent_sem.at[k]).wait()


def put_out(up_v, dn_v, out_v, up_out, dn_out, out, sem):
    copies = [pltpu.make_async_copy(out_v, out, sem.at[32])]
    for f in range(16):
        copies.append(pltpu.make_async_copy(dn_v.at[f], dn_out.at[:, pl.ds(128 * f, 128)], sem.at[f]))
    for k in range(16):
        rows, h = pl.ds(256 * (k // 2), 256), k % 2
        copies.append(pltpu.make_async_copy(up_v.at[h, rows], up_out.at[rows, pl.ds(512 * h, 512)], sem.at[16 + k]))
    for copy in copies:
        copy.start()
    for copy in copies:
        copy.wait()


def on_device(tokens, norm_gain, up_master, down_master):
    anywhere, vmem = pl.BlockSpec(memory_space=pl.ANY), pl.BlockSpec(memory_space=pltpu.VMEM)
    in_hbm = lambda v: pltpu.with_memory_space_constraint(v, pltpu.HBM)
    held = pl.pallas_call(
        kernel,
        name="gather_mlp",
        out_shape=(
            pltpu.VMEM((2, D, 512), BF),
            pltpu.VMEM((16, 1024, 128), BF),
            pltpu.VMEM((ROWS, 256), BF),
        ),
        in_specs=[anywhere] * 4,
        out_specs=(vmem, vmem, vmem),
        scratch_shapes=[
            pltpu.VMEM((128, 1024), F32),
            pltpu.VMEM((128, 1024), F32),
            pltpu.VMEM((1, 128), F32),
            pltpu.VMEM((8, ROWS, 256), BF),
            pltpu.VMEM((ROWS, 128), F32),
            pltpu.VMEM((2, ROWS, 512), F32),
            pltpu.VMEM((ROWS, 1024), BF),
            pltpu.VMEM((2, 4, ROWS, 256), BF),
            pltpu.VMEM((4, ROWS, 256), BF),
            pltpu.VMEM((2, 512, 256), BF),
            pltpu.VMEM((2, 512, 256), BF),
            pltpu.VMEM((2, ROWS, 256), BF),
            pltpu.SemaphoreType.DMA((4,)),
            pltpu.SemaphoreType.DMA((5,)),
            pltpu.SemaphoreType.DMA((2, 2, 22)),
            pltpu.SemaphoreType.DMA((11,)),
            pltpu.SemaphoreType.DMA((4, 2)),
            pltpu.SemaphoreType.DMA((12,)),
        ],
        compiler_params=pltpu.CompilerParams(collective_id=0, has_side_effects=True, vmem_limit_bytes=40 << 20),
    )(in_hbm(tokens), in_hbm(norm_gain.reshape(1, 128)), in_hbm(up_master), in_hbm(down_master))
    return pl.pallas_call(
        put_out,
        name="put_out",
        out_shape=(
            jax.ShapeDtypeStruct((D, 1024), BF),
            jax.ShapeDtypeStruct((1024, D), BF),
            jax.ShapeDtypeStruct((ROWS, 256), BF),
        ),
        in_specs=[vmem] * 3,
        out_specs=(anywhere,) * 3,
        scratch_shapes=[pltpu.SemaphoreType.DMA((33,))],
        compiler_params=pltpu.CompilerParams(vmem_limit_bytes=16 << 20),
    )(*held)


def solution(mesh):
    in_specs = (P("fs", "tp"), P("fs"), P("fs", "tp"), P("fs", "tp"))
    out_specs = (P(None, "tp"), P("tp", None), P("fs", "tp"))
    return jax.shard_map(
        on_device, mesh=mesh, in_specs=in_specs, out_specs=out_specs, check_vma=False
    )
```

```python
import jax
import jax.numpy as jnp
from jax import lax
from jax.experimental import pallas as pl
from jax.experimental.pallas import tpu as pltpu
from jax.sharding import PartitionSpec as P

norm_floor = 1e-06

MESH = pl.DeviceIdType.MESH
BF, F32 = jnp.bfloat16, jnp.float32
D, FF = 2048, 8192
ROWS = 1024
TILE = 512
UP, DN = 0, 1
GROUPS = (
    [(0, j, "G", s) for j in (0, "+") for s in (1, -1)],
    [(1, 0, "G", s) for s in ("+", "-")],
    [(0, 2, "T", 1, 1), (0, 2, "T", -1, 0)] + [(1, j, "G", s) for j in (1, -1) for s in ("+", "-")],
    [(0, j, "G", s) for j in ("-", 2) for s in (1, -1)] + [(1, 2, "T", "-", 0), (1, 2, "G", "+"), (1, 2, "G", "-")],
)


def kernel(
    tok_in, gain_in, up_in, dn_in,
    up_v, dn_v, out_v,
    up32, dn32, gain_v, tok_v, scale_v, acc, hid, pbuf, prx, fwd, qf, fin,
    in_sem, sent_sem, w_recv, t_recv, p_recv, r_recv,
):
    fs, tp = lax.axis_index("fs"), lax.axis_index("tp")
    z, y, x, c = fs // 4, fs % 4, tp // 2, tp % 2
    mod4 = lambda v: lax.rem(v + 8, 4)
    to_y = lambda s: {"fs": z * 4 + mod4(y + s), "tp": tp}
    to_z = lambda s: {"fs": mod4(z + s) * 4 + y, "tp": tp}
    to_x = lambda s: {"fs": fs, "tp": mod4(x + s) * 2 + c}
    partner = {"fs": fs, "tp": x * 2 + 1 - c}

    loads = [
        pltpu.make_async_copy(up_in, up32, in_sem.at[0]),
        pltpu.make_async_copy(gain_in, gain_v, in_sem.at[1]),
        pltpu.make_async_copy(tok_in, tok_v.at[tp], in_sem.at[2]),
        pltpu.make_async_copy(dn_in, dn32, in_sem.at[3]),
    ]
    loads[0].start()
    loads[1].start()
    barrier = pltpu.get_barrier_semaphore()
    for peer in (to_y(1), to_y(-1), to_z(1), to_z(-1), to_x(1), to_x(-1), partner):
        pl.semaphore_signal(barrier, inc=1, device_id=peer, device_id_type=MESH)

    def remote(src, dst, landed, send_sem, recv_sem, peer):
        out = lambda: pltpu.make_async_remote_copy(src, dst, send_sem, recv_sem, peer, MESH)
        back = lambda: pltpu.make_async_remote_copy(landed, landed, send_sem, recv_sem, peer, MESH)
        return out, back

    def go(pair):
        pair[0]().start()

    toward = 1 - 2 * (y % 2)
    y_at = {0: 0, "+": toward, "-": -toward, 2: 2}

    def weight_copies(w):
        def piece(h, jy, jz, q):
            f = mod4(z + jz) * 4 + mod4(y + y_at[jy])
            if w == UP:
                at, n = f * 128 + (0 if q is None else 64 * q), 128 if q is None else 64
                return up_v.at[h, pl.ds(pl.multiple_of(at, 64), n)]
            at, n = 512 * h + (0 if q is None else 256 * q), 512 if q is None else 256
            return dn_v.at[f, pl.ds(at, n)]

        tables, single = ({}, {}), [len(GROUPS)]

        def add(h, name, sent, side, landed):
            group = [g for g, names in enumerate(GROUPS) if (h, *name) in names]
            k = group[0] if group else single[0]
            single[0] += not group
            peer = to_y(y_at[side]) if side in ("+", "-") else to_z(side)
            src, got = piece(h, *sent), piece(h, *landed)
            tables[h][name] = remote(src, src, got, sent_sem.at[w], w_recv.at[w, k], peer)

        for s, other, q in (("+", "-", 1), ("-", "+", 0)):
            add(0, ("S", s), (0, 0, None), s, (s, 0, None))
            add(0, ("F", s), (other, 0, q), s, (2, 0, q))
            for jz in (0, 1, -1):
                add(1, (jz, "T", s), (0, jz, None), s, (s, jz, None))
                add(1, (jz, "G", s), (other, jz, q), s, (2, jz, q))
            for part in (0, 1):
                add(1, (2, "T", s, part), (0, 2, part), s, (s, 2, part))
            add(1, (2, "G", s), (other, 2, q), s, (2, 2, q))
        for s, q in ((1, 0), (-1, 1)):
            add(1, ("S", s), (0, 0, None), s, (0, -s, None))
            add(1, ("F", s), (0, -s, q), s, (0, 2, q))
            for jy in (0, "+", "-"):
                add(0, (jy, "T", s), (jy, 0, None), s, (jy, -s, None))
                add(0, (jy, "G", s), (jy, -s, q), s, (jy, 2, q))
            for part in (0, 1):
                add(0, (2, "T", s, part), (2, 0, part), s, (2, -s, part))
            add(0, (2, "G", s), (2, -s, q), s, (2, 2, q))
        return tables

    W = [weight_copies(w) for w in (UP, DN)]

    def take(w, h, *names):
        for name in names:
            W[w][h][name][1]().wait_recv()

    def take_group(w, g):
        n = len(GROUPS[g])
        if w == UP:
            ref = up_v.at[0, pl.ds(0, 64 * n)]
        else:
            ref = dn_v.at[pl.ds(0, n), pl.ds(0, 256)]
        pltpu.make_async_copy(ref, ref, w_recv.at[w, g]).wait()

    def put(w, h, *names):
        for name in names:
            go(W[w][h][name])

    def e0y(w):
        put(w, 0, ("S", "+"), ("S", "-"))
        put(w, 1, (0, "T", "+"), (0, "T", "-"))

    def e0z(w):
        put(w, 1, ("S", 1), ("S", -1))
        put(w, 0, (0, "T", 1), (0, "T", -1))

    def e1(w):
        take(w, 0, ("S", "+"))
        put(w, 0, ("+", "T", 1), ("+", "T", -1), ("F", "-"))
        for s in (1, -1):
            take(w, 1, ("S", s))
            put(w, 1, (-s, "T", "+"), (-s, "T", "-"), ("F", s))
        take(w, 0, ("S", "-"))
        put(w, 0, ("F", "+"))

    def e2(w):
        for s in (1, -1):
            take(w, 0, (0, "T", s))
            put(w, 0, (0, "G", s))
        take(w, 1, (0, "T", "+"))
        put(w, 1, (0, "G", "-"))
        take(w, 1, (0, "T", "-"))

    def e3a(w):
        for s in (1, -1):
            take(w, 0, ("+", "T", s))
            put(w, 0, ("+", "G", s))

    def e3b(w):
        for s, q in ((1, 0), (-1, 1)):
            take(w, 1, ("F", s))
            put(w, 1, (2, "T", "+", q), (2, "T", "-", q))
        put(w, 0, ("-", "T", 1), ("-", "T", -1))
        put(w, 1, (0, "G", "+"))

    def e3c(w):
        for s, q in (("-", 0), ("+", 1)):
            take(w, 0, ("F", s))
            put(w, 0, (2, "T", 1, q), (2, "T", -1, q))

    def e4a(w, sides=(-1, 1)):
        for jz in sides:
            for s, other in (("+", "-"), ("-", "+")):
                take(w, 1, (jz, "T", s))
                put(w, 1, (jz, "G", other))

    def own_far(w):
        take_group(w, 0)
        take(w, 1, (2, "T", "+", 0))
        put(w, 1, (2, "G", "-"))
        take(w, 1, (2, "T", "+", 1))

    def e4b(w):
        take(w, 1, (2, "T", "-", 1))
        put(w, 1, (2, "G", "+"))

    def e4c(w):
        for s in (1, -1):
            take(w, 0, ("-", "T", s))
            put(w, 0, ("-", "G", s))

    def e4d(w):
        for s, q in ((1, 0), (-1, 1)):
            take(w, 0, (2, "T", s, q))
            put(w, 0, (2, "G", s))

    def other_near(w):
        take_group(w, 1)

    def other_side(w):
        take_group(w, 2)

    def other_far(w):
        take_group(w, 3)

    def rows_of(t, half):
        return tok_v.at[t] if half is None else tok_v.at[t, pl.ds(512 * half, 512)]

    block = lambda d, core: mod4(x + d) * 2 + core
    T = {}

    def token_copy(name, d_sent, half, peer, d_landed, core_landed):
        k = min(len(T), 6)
        sent, got = rows_of(block(d_sent, c), half), rows_of(block(d_landed, core_landed), half)
        T[name] = remote(sent, sent, got, sent_sem.at[2], t_recv.at[k], peer)

    for half in (0, 1):
        token_copy(("X+", half), 0, half, to_x(1), -1, c)
        token_copy(("X-", half), 0, half, to_x(-1), 1, c)
    token_copy("Y+", -1, 0, to_x(1), 2, c)
    token_copy("Y-", 1, 1, to_x(-1), 2, c)
    token_copy(("D", 0), 0, None, partner, 0, 1 - c)
    token_copy(("D", -1), -1, None, partner, -1, 1 - c)
    token_copy(("D", 1), 1, None, partner, 1, 1 - c)
    token_copy(("D", 2, 0), 2, 0, partner, 2, 1 - c)
    token_copy(("D", 2, 1), 2, 1, partner, 2, 1 - c)

    loads[0].wait()
    loads[2].start()
    loads[3].start()
    loads[1].wait()
    gain = jnp.transpose(jnp.broadcast_to(gain_v[...], (128, 128)))
    for h in (0, 1):
        for k in range(4):
            cols = slice(512 * h + 128 * k, 512 * h + 128 * k + 128)
            up_v[h, pl.ds(pl.multiple_of(fs * 128, 128), 128), 128 * k : 128 * k + 128] = (gain * up32[:, cols]).astype(BF)
    pl.semaphore_wait(barrier, 7)

    e0y(UP)
    e0z(UP)
    loads[2].wait()
    go(T["X+", 0]), go(T["X-", 1]), go(T["X+", 1]), go(T["X-", 0])
    go(T["D", 0])

    loads[3].wait()
    for k in range(8):
        dn_v[fs, 128 * k : 128 * k + 128, :] = jnp.transpose(dn32[:, 128 * k : 128 * k + 128]).astype(BF)

    e1(UP)
    e2(UP)
    T["X+", 0][1]().wait_recv()
    go(T["Y+"])
    T["X-", 1][1]().wait_recv()
    go(T["Y-"])
    e3a(UP)
    e3b(UP)
    T["X+", 1][1]().wait_recv()
    go(T["D", -1])
    T["X-", 0][1]().wait_recv()
    go(T["D", 1])
    e4a(UP)
    e3c(UP)
    e4c(UP)
    own_far(UP)
    T["Y+"][1]().wait_recv()
    go(T["D", 2, 0])
    T["Y-"][1]().wait_recv()
    go(T["D", 2, 1])
    e4b(UP)
    e0y(DN)
    e4d(UP)
    e0z(DN)
    pltpu.make_async_copy(tok_v.at[pl.ds(0, 4)], tok_v.at[pl.ds(0, 4)], t_recv.at[6]).wait()

    ones = jnp.ones((128, 128), BF)

    def factor(m, carry):
        rows = pl.ds(pl.multiple_of(m * 256, 256), 256)
        total = jnp.zeros((256, 128), F32)
        for t in range(8):
            v = tok_v[t, rows, :].astype(F32)
            total += v[:, :128] * v[:, :128] + v[:, 128:] * v[:, 128:]
        high = total.astype(BF)
        low = (total - high.astype(F32)).astype(BF)
        summed = jnp.dot(high, ones, preferred_element_type=F32) + jnp.dot(low, ones, preferred_element_type=F32)
        scale_v[rows, :] = lax.rsqrt(summed * (1.0 / D) + norm_floor)
        return carry

    lax.fori_loop(0, ROWS // 256, factor, 0)

    near = y // 2

    def core_of(o):
        return near if o == 0 else 1 - near

    def pair_of(dz, o):
        return mod4(z + dz) * 2 + core_of(o)

    def dots(h, rows, pairs):
        total = None
        for pair in pairs:
            t = pair_of(*pair)
            weights = up_v[h, pl.ds(pl.multiple_of(256 * t, 256), 256), :]
            term = jnp.dot(tok_v[t, rows, :], weights, preferred_element_type=F32)
            total = term if total is None else total + term
        return total

    def first_part(i, carry):
        h, m = i // (ROWS // TILE), lax.rem(i, ROWS // TILE)
        rows = pl.ds(pl.multiple_of(m * TILE, TILE), TILE)
        acc[h, rows, :] = dots(h, rows, ((0, 0), (1, 0), (3, 0), (2, 0)))
        return carry

    def second_part(h):
        def tile(m, carry):
            rows = pl.ds(pl.multiple_of(m * TILE, TILE), TILE)
            total = acc[h, rows, :] + dots(h, rows, ((0, 1), (1, 1), (3, 1), (2, 1)))
            factor_of = scale_v[rows, :]
            for k in range(4):
                v = jnp.maximum(total[:, 128 * k : 128 * k + 128] * factor_of, 0.0)
                hid[rows, 512 * h + 128 * k : 512 * h + 128 * k + 128] = (v * v).astype(BF)
            return carry

        lax.fori_loop(0, ROWS // TILE, tile, 0)

    lax.fori_loop(0, 2 * ROWS // TILE, first_part, 0)
    other_near(UP)
    other_side(UP)
    other_far(UP)
    second_part(0)
    e1(DN)
    second_part(1)
    e2(DN)

    def remote_partial(dz, o, r):
        part = pl.ds(pl.multiple_of(512 * r, 512), 512)
        return remote(pbuf.at[o, dz, part], prx.at[dz, part], prx.at[dz, part], sent_sem.at[3], p_recv.at[dz, r], partner)

    def product(dz, o):
        t = pair_of(dz, o)

        def tile(r, carry):
            rows = pl.ds(pl.multiple_of(r * 512, 512), 512)
            pair = jnp.concatenate([dn_v[2 * t], dn_v[2 * t + 1]], axis=1)
            pbuf[o, dz, rows, :] = jnp.dot(hid[rows, :], pair, preferred_element_type=F32).astype(BF)

            @pl.when(core_of(o) != c)
            def _():
                remote_partial(dz, o, r)[0]().start()

            return carry

        lax.fori_loop(0, 2, tile, 0)

    def ring(sign):
        side = 0 if sign == 1 else 1
        q, k, peer = side, 2 * side, to_x(sign)
        chunk = lambda ref, base, j: ref.at[pl.ds(base + 256 * j, 256)]

        def first(src, j):
            got = chunk(fwd.at[side], 0, j)
            return remote(chunk(src, 512 * q, j), got, got, sent_sem.at[4], r_recv.at[k + j], peer)

        def second(j):
            got = chunk(fin.at[side], 512 * q, j)
            return remote(chunk(qf.at[side], 0, j), got, got, sent_sem.at[4], r_recv.at[4], peer)

        def direct(src, j):
            got = chunk(fin.at[side], 512 * (1 - q), j)
            return remote(chunk(src, 512 * (1 - q), j), got, got, sent_sem.at[4], r_recv.at[4], peer)

        return first, second, direct

    RING = {1: ring(1), -1: ring(-1)}
    ahead = lambda dz: mod4(z + dz - x)

    def reduce_pair(dz, o):
        @pl.when(core_of(o) == c)
        def _():
            mine = pbuf.at[o, dz]
            for r, sign, d in ((0, 1, 3), (1, -1, 1)):
                remote_partial(dz, o, r)[1]().wait_recv()
                rows = pl.ds(512 * r, 512)
                pbuf[o, dz, rows, :] = (pbuf[o, dz, rows, :].astype(F32) + prx[dz, rows, :].astype(F32)).astype(BF)

                @pl.when(ahead(dz) == 2)
                def _():
                    RING[sign][0](mine, 0)[0]().start()
                    RING[sign][0](mine, 1)[0]().start()

                @pl.when(ahead(dz) == d)
                def _():
                    RING[-sign][2](mine, 0)[0]().start()
                    if not later(dz, o):
                        RING[-sign][2](mine, 1)[0]().start()

    later = lambda dz, o: o == 1 and dz in (1, 3)

    def direct_rest(dz, o):
        @pl.when(core_of(o) == c)
        def _():
            for sign, d in ((1, 1), (-1, 3)):
                @pl.when(ahead(dz) == d)
                def _():
                    RING[sign][2](pbuf.at[o, dz], 1)[0]().start()

    def forward(dz, o):
        @pl.when(core_of(o) == c)
        def _():
            for sign, d in ((1, 1), (-1, 3)):
                side = 0 if sign == 1 else 1

                @pl.when(ahead(dz) == d)
                def _():
                    for j in (0, 1):
                        RING[sign][0](pbuf.at[o, dz], j)[1]().wait_recv()
                        here, mine = pl.ds(256 * j, 256), pl.ds(512 * side + 256 * j, 256)
                        qf[side, here, :] = (pbuf[o, dz, mine, :].astype(F32) + fwd[side, here, :].astype(F32)).astype(BF)
                        RING[sign][1](j)[0]().start()

    product(0, 0)
    e3a(DN)
    reduce_pair(0, 0)
    e4a(DN, (-1,))
    product(3, 0)
    e3b(DN)
    reduce_pair(3, 0)
    e4a(DN, (1,))
    product(1, 0)
    e3c(DN)
    reduce_pair(1, 0)
    forward(0, 0)
    own_far(DN)
    product(2, 0)
    e4c(DN)
    reduce_pair(2, 0)
    e4b(DN)
    forward(3, 0)
    other_near(DN)
    product(0, 1)
    e4d(DN)
    other_side(DN)
    product(1, 1)
    reduce_pair(0, 1)
    product(3, 1)
    forward(1, 0)
    reduce_pair(1, 1)
    reduce_pair(3, 1)
    other_far(DN)
    product(2, 1)
    forward(2, 0)
    reduce_pair(2, 1)
    direct_rest(1, 1)
    direct_rest(3, 1)
    forward(0, 1)
    forward(1, 1)
    forward(3, 1)
    forward(2, 1)

    mine = mod4(x - z)
    o_mine = jnp.where(near == c, 0, 1)
    pltpu.make_async_copy(fin, fin, r_recv.at[4]).wait()

    def last(m, carry):
        rows = pl.ds(pl.multiple_of(m * TILE, TILE), TILE)
        total = pbuf[o_mine, mine, rows, :].astype(F32) + fin[0, rows, :].astype(F32) + fin[1, rows, :].astype(F32)
        out_v[rows, :] = total.astype(BF)
        return carry

    lax.fori_loop(0, ROWS // TILE, last, 0)

    for k, ref in enumerate((up_v.at[:, pl.ds(0, 1920)], dn_v.at[pl.ds(0, 15)], tok_v.at[pl.ds(0, 7)], prx, pbuf.at[0, pl.ds(0, 3)])):
        pltpu.make_async_copy(ref, ref, sent_sem.at[k]).wait()


def put_out(up_v, dn_v, out_v, up_out, dn_out, out, sem):
    copies = [pltpu.make_async_copy(out_v, out, sem.at[32])]
    for f in range(16):
        copies.append(pltpu.make_async_copy(dn_v.at[f], dn_out.at[:, pl.ds(128 * f, 128)], sem.at[f]))
    for k in range(16):
        rows, h = pl.ds(256 * (k // 2), 256), k % 2
        copies.append(pltpu.make_async_copy(up_v.at[h, rows], up_out.at[rows, pl.ds(512 * h, 512)], sem.at[16 + k]))
    for copy in copies:
        copy.start()
    for copy in copies:
        copy.wait()


def on_device(tokens, norm_gain, up_master, down_master):
    anywhere, vmem = pl.BlockSpec(memory_space=pl.ANY), pl.BlockSpec(memory_space=pltpu.VMEM)
    in_hbm = lambda v: pltpu.with_memory_space_constraint(v, pltpu.HBM)
    held = pl.pallas_call(
        kernel,
        name="gather_mlp",
        out_shape=(
            pltpu.VMEM((2, D, 512), BF),
            pltpu.VMEM((16, 1024, 128), BF),
            pltpu.VMEM((ROWS, 256), BF),
        ),
        in_specs=[anywhere] * 4,
        out_specs=(vmem, vmem, vmem),
        scratch_shapes=[
            pltpu.VMEM((128, 1024), F32),
            pltpu.VMEM((128, 1024), F32),
            pltpu.VMEM((1, 128), F32),
            pltpu.VMEM((8, ROWS, 256), BF),
            pltpu.VMEM((ROWS, 128), F32),
            pltpu.VMEM((2, ROWS, 512), F32),
            pltpu.VMEM((ROWS, 1024), BF),
            pltpu.VMEM((2, 4, ROWS, 256), BF),
            pltpu.VMEM((4, ROWS, 256), BF),
            pltpu.VMEM((2, 512, 256), BF),
            pltpu.VMEM((2, 512, 256), BF),
            pltpu.VMEM((2, ROWS, 256), BF),
            pltpu.SemaphoreType.DMA((4,)),
            pltpu.SemaphoreType.DMA((5,)),
            pltpu.SemaphoreType.DMA((2, 29)),
            pltpu.SemaphoreType.DMA((7,)),
            pltpu.SemaphoreType.DMA((4, 2)),
            pltpu.SemaphoreType.DMA((5,)),
        ],
        compiler_params=pltpu.CompilerParams(collective_id=0, has_side_effects=True, vmem_limit_bytes=40 << 20),
    )(in_hbm(tokens), in_hbm(norm_gain.reshape(1, 128)), in_hbm(up_master), in_hbm(down_master))
    return pl.pallas_call(
        put_out,
        name="put_out",
        out_shape=(
            jax.ShapeDtypeStruct((D, 1024), BF),
            jax.ShapeDtypeStruct((1024, D), BF),
            jax.ShapeDtypeStruct((ROWS, 256), BF),
        ),
        in_specs=[vmem] * 3,
        out_specs=(anywhere,) * 3,
        scratch_shapes=[pltpu.SemaphoreType.DMA((33,))],
        compiler_params=pltpu.CompilerParams(vmem_limit_bytes=16 << 20),
    )(*held)


def solution(mesh):
    in_specs = (P("fs", "tp"), P("fs"), P("fs", "tp"), P("fs", "tp"))
    out_specs = (P(None, "tp"), P("tp", None), P("fs", "tp"))
    return jax.shard_map(
        on_device, mesh=mesh, in_specs=in_specs, out_specs=out_specs, check_vma=False
    )
```

```python
import jax
import jax.numpy as jnp
from jax import lax
from jax.experimental import pallas as pl
from jax.experimental.pallas import tpu as pltpu
from jax.sharding import PartitionSpec as P

norm_floor = 1e-06

MESH = pl.DeviceIdType.MESH
BF, F32 = jnp.bfloat16, jnp.float32
D, FF = 2048, 8192
ROWS = 1024
TILE = 512
UP, DN = 0, 1
GROUPS = (
    [(0, j, "G", s) for j in (0, "+") for s in (1, -1)],
    [(1, 0, "G", s) for s in ("+", "-")],
    [(0, 2, "T", 1, 1), (0, 2, "T", -1, 0)] + [(1, j, "G", s) for j in (1, -1) for s in ("+", "-")],
    [(0, j, "G", s) for j in ("-", 2) for s in (1, -1)] + [(1, 2, "T", "-", 0), (1, 2, "G", "+"), (1, 2, "G", "-")],
)


def kernel(
    tok_in, gain_in, up_in, dn_in,
    up_v, dn_v, own_v, fin,
    up32, dn32, gain_v, tok_v, scale_v, acc, hid, pbuf, prx, fwd, qf,
    in_sem, sent_sem, w_recv, t_recv, p_recv, r_recv,
):
    fs, tp = lax.axis_index("fs"), lax.axis_index("tp")
    z, y, x, c = fs // 4, fs % 4, tp // 2, tp % 2
    mod4 = lambda v: lax.rem(v + 8, 4)
    to_y = lambda s: {"fs": z * 4 + mod4(y + s), "tp": tp}
    to_z = lambda s: {"fs": mod4(z + s) * 4 + y, "tp": tp}
    to_x = lambda s: {"fs": fs, "tp": mod4(x + s) * 2 + c}
    partner = {"fs": fs, "tp": x * 2 + 1 - c}

    loads = [
        pltpu.make_async_copy(up_in, up32, in_sem.at[0]),
        pltpu.make_async_copy(gain_in, gain_v, in_sem.at[1]),
        pltpu.make_async_copy(tok_in, tok_v.at[tp], in_sem.at[2]),
        pltpu.make_async_copy(dn_in, dn32, in_sem.at[3]),
    ]
    loads[0].start()
    loads[1].start()
    barrier = pltpu.get_barrier_semaphore()
    for peer in (to_y(1), to_y(-1), to_z(1), to_z(-1), to_x(1), to_x(-1), partner):
        pl.semaphore_signal(barrier, inc=1, device_id=peer, device_id_type=MESH)

    def remote(src, dst, landed, send_sem, recv_sem, peer):
        out = lambda: pltpu.make_async_remote_copy(src, dst, send_sem, recv_sem, peer, MESH)
        back = lambda: pltpu.make_async_remote_copy(landed, landed, send_sem, recv_sem, peer, MESH)
        return out, back

    def go(pair):
        pair[0]().start()

    toward = 1 - 2 * (y % 2)
    y_at = {0: 0, "+": toward, "-": -toward, 2: 2}

    def weight_copies(w):
        def piece(h, jy, jz, q):
            f = mod4(z + jz) * 4 + mod4(y + y_at[jy])
            if w == UP:
                at, n = f * 128 + (0 if q is None else 64 * q), 128 if q is None else 64
                return up_v.at[h, pl.ds(pl.multiple_of(at, 64), n)]
            at, n = 512 * h + (0 if q is None else 256 * q), 512 if q is None else 256
            return dn_v.at[f, pl.ds(at, n)]

        tables, single = ({}, {}), [len(GROUPS)]

        def add(h, name, sent, side, landed):
            group = [g for g, names in enumerate(GROUPS) if (h, *name) in names]
            k = group[0] if group else single[0]
            single[0] += not group
            peer = to_y(y_at[side]) if side in ("+", "-") else to_z(side)
            src, got = piece(h, *sent), piece(h, *landed)
            tables[h][name] = remote(src, src, got, sent_sem.at[w], w_recv.at[w, k], peer)

        for s, other, q in (("+", "-", 1), ("-", "+", 0)):
            add(0, ("S", s), (0, 0, None), s, (s, 0, None))
            add(0, ("F", s), (other, 0, q), s, (2, 0, q))
            for jz in (0, 1, -1):
                add(1, (jz, "T", s), (0, jz, None), s, (s, jz, None))
                add(1, (jz, "G", s), (other, jz, q), s, (2, jz, q))
            for part in (0, 1):
                add(1, (2, "T", s, part), (0, 2, part), s, (s, 2, part))
            add(1, (2, "G", s), (other, 2, q), s, (2, 2, q))
        for s, q in ((1, 0), (-1, 1)):
            add(1, ("S", s), (0, 0, None), s, (0, -s, None))
            add(1, ("F", s), (0, -s, q), s, (0, 2, q))
            for jy in (0, "+", "-"):
                add(0, (jy, "T", s), (jy, 0, None), s, (jy, -s, None))
                add(0, (jy, "G", s), (jy, -s, q), s, (jy, 2, q))
            for part in (0, 1):
                add(0, (2, "T", s, part), (2, 0, part), s, (2, -s, part))
            add(0, (2, "G", s), (2, -s, q), s, (2, 2, q))
        return tables

    W = [weight_copies(w) for w in (UP, DN)]

    def take(w, h, *names):
        for name in names:
            W[w][h][name][1]().wait_recv()

    def take_group(w, g):
        n = len(GROUPS[g])
        if w == UP:
            ref = up_v.at[0, pl.ds(0, 64 * n)]
        else:
            ref = dn_v.at[pl.ds(0, n), pl.ds(0, 256)]
        pltpu.make_async_copy(ref, ref, w_recv.at[w, g]).wait()

    def put(w, h, *names):
        for name in names:
            go(W[w][h][name])

    def e0y(w):
        put(w, 0, ("S", "+"), ("S", "-"))
        put(w, 1, (0, "T", "+"), (0, "T", "-"))

    def e0z(w):
        put(w, 1, ("S", 1), ("S", -1))
        put(w, 0, (0, "T", 1), (0, "T", -1))

    def e1(w):
        take(w, 0, ("S", "+"))
        put(w, 0, ("+", "T", 1), ("+", "T", -1), ("F", "-"))
        for s in (1, -1):
            take(w, 1, ("S", s))
            put(w, 1, (-s, "T", "+"), (-s, "T", "-"), ("F", s))
        take(w, 0, ("S", "-"))
        put(w, 0, ("F", "+"))

    def e2(w):
        for s in (1, -1):
            take(w, 0, (0, "T", s))
            put(w, 0, (0, "G", s))
        take(w, 1, (0, "T", "+"))
        put(w, 1, (0, "G", "-"))
        take(w, 1, (0, "T", "-"))

    def e3a(w):
        for s in (1, -1):
            take(w, 0, ("+", "T", s))
            put(w, 0, ("+", "G", s))

    def e3b(w):
        for s, q in ((1, 0), (-1, 1)):
            take(w, 1, ("F", s))
            put(w, 1, (2, "T", "+", q), (2, "T", "-", q))
        put(w, 0, ("-", "T", 1), ("-", "T", -1))
        put(w, 1, (0, "G", "+"))

    def e3c(w):
        for s, q in (("-", 0), ("+", 1)):
            take(w, 0, ("F", s))
            put(w, 0, (2, "T", 1, q), (2, "T", -1, q))

    def e4a(w, sides=(-1, 1)):
        for jz in sides:
            for s, other in (("+", "-"), ("-", "+")):
                take(w, 1, (jz, "T", s))
                put(w, 1, (jz, "G", other))

    def own_far(w):
        take_group(w, 0)
        take(w, 1, (2, "T", "+", 0))
        put(w, 1, (2, "G", "-"))
        take(w, 1, (2, "T", "+", 1))

    def e4b(w):
        take(w, 1, (2, "T", "-", 1))
        put(w, 1, (2, "G", "+"))

    def e4c(w):
        for s in (1, -1):
            take(w, 0, ("-", "T", s))
            put(w, 0, ("-", "G", s))

    def e4d(w):
        for s, q in ((1, 0), (-1, 1)):
            take(w, 0, (2, "T", s, q))
            put(w, 0, (2, "G", s))

    def other_near(w):
        take_group(w, 1)

    def other_side(w):
        take_group(w, 2)

    def other_far(w):
        take_group(w, 3)

    def rows_of(t, half):
        return tok_v.at[t] if half is None else tok_v.at[t, pl.ds(512 * half, 512)]

    block = lambda d, core: mod4(x + d) * 2 + core
    T = {}

    def token_copy(name, d_sent, half, peer, d_landed, core_landed):
        k = min(len(T), 6)
        sent, got = rows_of(block(d_sent, c), half), rows_of(block(d_landed, core_landed), half)
        T[name] = remote(sent, sent, got, sent_sem.at[2], t_recv.at[k], peer)

    for half in (0, 1):
        token_copy(("X+", half), 0, half, to_x(1), -1, c)
        token_copy(("X-", half), 0, half, to_x(-1), 1, c)
    token_copy("Y+", -1, 0, to_x(1), 2, c)
    token_copy("Y-", 1, 1, to_x(-1), 2, c)
    token_copy(("D", 0), 0, None, partner, 0, 1 - c)
    token_copy(("D", -1), -1, None, partner, -1, 1 - c)
    token_copy(("D", 1), 1, None, partner, 1, 1 - c)
    token_copy(("D", 2, 0), 2, 0, partner, 2, 1 - c)
    token_copy(("D", 2, 1), 2, 1, partner, 2, 1 - c)

    loads[0].wait()
    loads[2].start()
    loads[3].start()
    loads[1].wait()
    gain = jnp.transpose(jnp.broadcast_to(gain_v[...], (128, 128)))
    for h in (0, 1):
        for k in range(4):
            cols = slice(512 * h + 128 * k, 512 * h + 128 * k + 128)
            up_v[h, pl.ds(pl.multiple_of(fs * 128, 128), 128), 128 * k : 128 * k + 128] = (gain * up32[:, cols]).astype(BF)
    pl.semaphore_wait(barrier, 7)

    e0y(UP)
    e0z(UP)
    loads[2].wait()
    go(T["X+", 0]), go(T["X-", 1]), go(T["X+", 1]), go(T["X-", 0])
    go(T["D", 0])

    loads[3].wait()
    for k in range(8):
        dn_v[fs, 128 * k : 128 * k + 128, :] = jnp.transpose(dn32[:, 128 * k : 128 * k + 128]).astype(BF)

    e1(UP)
    e2(UP)
    T["X+", 0][1]().wait_recv()
    go(T["Y+"])
    T["X-", 1][1]().wait_recv()
    go(T["Y-"])
    e3a(UP)
    e3b(UP)
    T["X+", 1][1]().wait_recv()
    go(T["D", -1])
    T["X-", 0][1]().wait_recv()
    go(T["D", 1])
    e4a(UP)
    e3c(UP)
    e4c(UP)
    own_far(UP)
    T["Y+"][1]().wait_recv()
    go(T["D", 2, 0])
    T["Y-"][1]().wait_recv()
    go(T["D", 2, 1])
    e4b(UP)
    e0y(DN)
    e4d(UP)
    e0z(DN)
    pltpu.make_async_copy(tok_v.at[pl.ds(0, 4)], tok_v.at[pl.ds(0, 4)], t_recv.at[6]).wait()

    ones = jnp.ones((128, 128), BF)

    def factor(m, carry):
        rows = pl.ds(pl.multiple_of(m * 256, 256), 256)
        total = jnp.zeros((256, 128), F32)
        for t in range(8):
            v = tok_v[t, rows, :].astype(F32)
            total += v[:, :128] * v[:, :128] + v[:, 128:] * v[:, 128:]
        high = total.astype(BF)
        low = (total - high.astype(F32)).astype(BF)
        summed = jnp.dot(high, ones, preferred_element_type=F32) + jnp.dot(low, ones, preferred_element_type=F32)
        scale_v[rows, :] = lax.rsqrt(summed * (1.0 / D) + norm_floor)
        return carry

    lax.fori_loop(0, ROWS // 256, factor, 0)

    near = y // 2

    def core_of(o):
        return near if o == 0 else 1 - near

    def pair_of(dz, o):
        return mod4(z + dz) * 2 + core_of(o)

    def dots(h, rows, pairs):
        total = None
        for pair in pairs:
            t = pair_of(*pair)
            weights = up_v[h, pl.ds(pl.multiple_of(256 * t, 256), 256), :]
            term = jnp.dot(tok_v[t, rows, :], weights, preferred_element_type=F32)
            total = term if total is None else total + term
        return total

    def first_part(i, carry):
        h, m = i // (ROWS // TILE), lax.rem(i, ROWS // TILE)
        rows = pl.ds(pl.multiple_of(m * TILE, TILE), TILE)
        acc[h, rows, :] = dots(h, rows, ((0, 0), (1, 0), (3, 0), (2, 0)))
        return carry

    def second_part(h):
        def tile(m, carry):
            rows = pl.ds(pl.multiple_of(m * TILE, TILE), TILE)
            total = acc[h, rows, :] + dots(h, rows, ((0, 1), (1, 1), (3, 1), (2, 1)))
            factor_of = scale_v[rows, :]
            for k in range(4):
                v = jnp.maximum(total[:, 128 * k : 128 * k + 128] * factor_of, 0.0)
                hid[rows, 512 * h + 128 * k : 512 * h + 128 * k + 128] = (v * v).astype(BF)
            return carry

        lax.fori_loop(0, ROWS // TILE, tile, 0)

    lax.fori_loop(0, 2 * ROWS // TILE, first_part, 0)
    other_near(UP)
    other_side(UP)
    other_far(UP)
    second_part(0)
    e1(DN)
    second_part(1)
    e2(DN)

    def remote_partial(dz, o, r):
        part = pl.ds(pl.multiple_of(512 * r, 512), 512)
        return remote(pbuf.at[o, dz, part], prx.at[dz, part], prx.at[dz, part], sent_sem.at[3], p_recv.at[dz, r], partner)

    def product(dz, o):
        t = pair_of(dz, o)

        def tile(r, carry):
            rows = pl.ds(pl.multiple_of(r * 512, 512), 512)
            pair = jnp.concatenate([dn_v[2 * t], dn_v[2 * t + 1]], axis=1)
            pbuf[o, dz, rows, :] = jnp.dot(hid[rows, :], pair, preferred_element_type=F32).astype(BF)

            @pl.when(core_of(o) != c)
            def _():
                remote_partial(dz, o, r)[0]().start()

            return carry

        lax.fori_loop(0, 2, tile, 0)

    def ring(sign):
        side = 0 if sign == 1 else 1
        q, k, peer = side, 2 * side, to_x(sign)
        chunk = lambda ref, base, j: ref.at[pl.ds(base + 256 * j, 256)]

        def first(src, j):
            got = chunk(fwd.at[side], 0, j)
            return remote(chunk(src, 512 * q, j), got, got, sent_sem.at[4], r_recv.at[k + j], peer)

        def second(j):
            got = chunk(fin.at[side], 512 * q, j)
            return remote(chunk(qf.at[side], 0, j), got, got, sent_sem.at[4], r_recv.at[4], peer)

        def direct(src, j):
            got = chunk(fin.at[side], 512 * (1 - q), j)
            return remote(chunk(src, 512 * (1 - q), j), got, got, sent_sem.at[4], r_recv.at[4], peer)

        return first, second, direct

    RING = {1: ring(1), -1: ring(-1)}
    ahead = lambda dz: mod4(z + dz - x)

    def reduce_pair(dz, o):
        @pl.when(core_of(o) == c)
        def _():
            mine = pbuf.at[o, dz]
            for r, sign, d in ((0, 1, 3), (1, -1, 1)):
                remote_partial(dz, o, r)[1]().wait_recv()
                rows = pl.ds(512 * r, 512)
                pbuf[o, dz, rows, :] = (pbuf[o, dz, rows, :].astype(F32) + prx[dz, rows, :].astype(F32)).astype(BF)

                @pl.when(ahead(dz) == 0)
                def _():
                    own_v[rows, :] = pbuf[o, dz, rows, :]

                @pl.when(ahead(dz) == 2)
                def _():
                    RING[sign][0](mine, 0)[0]().start()
                    RING[sign][0](mine, 1)[0]().start()

                @pl.when(ahead(dz) == d)
                def _():
                    RING[-sign][2](mine, 0)[0]().start()
                    if not later(dz, o):
                        RING[-sign][2](mine, 1)[0]().start()

    later = lambda dz, o: o == 1 and dz in (1, 3)

    def direct_rest(dz, o):
        @pl.when(core_of(o) == c)
        def _():
            for sign, d in ((1, 1), (-1, 3)):
                @pl.when(ahead(dz) == d)
                def _():
                    RING[sign][2](pbuf.at[o, dz], 1)[0]().start()

    def forward(dz, o):
        @pl.when(core_of(o) == c)
        def _():
            for sign, d in ((1, 1), (-1, 3)):
                side = 0 if sign == 1 else 1

                @pl.when(ahead(dz) == d)
                def _():
                    for j in (0, 1):
                        RING[sign][0](pbuf.at[o, dz], j)[1]().wait_recv()
                        here, mine = pl.ds(256 * j, 256), pl.ds(512 * side + 256 * j, 256)
                        qf[side, here, :] = (pbuf[o, dz, mine, :].astype(F32) + fwd[side, here, :].astype(F32)).astype(BF)
                        RING[sign][1](j)[0]().start()

    product(0, 0)
    e3a(DN)
    reduce_pair(0, 0)
    e4a(DN, (-1,))
    product(3, 0)
    e3b(DN)
    reduce_pair(3, 0)
    e4a(DN, (1,))
    product(1, 0)
    e3c(DN)
    reduce_pair(1, 0)
    forward(0, 0)
    own_far(DN)
    product(2, 0)
    e4c(DN)
    reduce_pair(2, 0)
    e4b(DN)
    forward(3, 0)
    other_near(DN)
    product(0, 1)
    e4d(DN)
    other_side(DN)
    product(1, 1)
    reduce_pair(0, 1)
    product(3, 1)
    forward(1, 0)
    reduce_pair(1, 1)
    reduce_pair(3, 1)
    other_far(DN)
    product(2, 1)
    forward(2, 0)
    reduce_pair(2, 1)
    direct_rest(1, 1)
    direct_rest(3, 1)
    forward(0, 1)
    forward(1, 1)
    forward(3, 1)
    forward(2, 1)

    pltpu.make_async_copy(fin, fin, r_recv.at[4]).wait()

    for k, ref in enumerate((up_v.at[:, pl.ds(0, 1920)], dn_v.at[pl.ds(0, 15)], tok_v.at[pl.ds(0, 7)], prx, pbuf.at[0, pl.ds(0, 3)])):
        pltpu.make_async_copy(ref, ref, sent_sem.at[k]).wait()


def put_out(up_v, dn_v, own_v, fin, up_out, dn_out, out, out_v, sem):
    copies = []
    for f in range(16):
        copies.append(pltpu.make_async_copy(dn_v.at[f], dn_out.at[:, pl.ds(128 * f, 128)], sem.at[f]))
    for k in range(16):
        rows, h = pl.ds(256 * (k // 2), 256), k % 2
        copies.append(pltpu.make_async_copy(up_v.at[h, rows], up_out.at[rows, pl.ds(512 * h, 512)], sem.at[16 + k]))
    for copy in copies:
        copy.start()
    for m in range(ROWS // 256):
        rows = pl.ds(256 * m, 256)
        total = own_v[rows, :].astype(F32) + fin[0, rows, :].astype(F32) + fin[1, rows, :].astype(F32)
        out_v[rows, :] = total.astype(BF)
    copies.append(pltpu.make_async_copy(out_v, out, sem.at[32]))
    copies[-1].start()
    for copy in copies:
        copy.wait()


def on_device(tokens, norm_gain, up_master, down_master):
    anywhere, vmem = pl.BlockSpec(memory_space=pl.ANY), pl.BlockSpec(memory_space=pltpu.VMEM)
    in_hbm = lambda v: pltpu.with_memory_space_constraint(v, pltpu.HBM)
    held = pl.pallas_call(
        kernel,
        name="gather_mlp",
        out_shape=(
            pltpu.VMEM((2, D, 512), BF),
            pltpu.VMEM((16, 1024, 128), BF),
            pltpu.VMEM((ROWS, 256), BF),
            pltpu.VMEM((2, ROWS, 256), BF),
        ),
        in_specs=[anywhere] * 4,
        out_specs=(vmem,) * 4,
        scratch_shapes=[
            pltpu.VMEM((128, 1024), F32),
            pltpu.VMEM((128, 1024), F32),
            pltpu.VMEM((1, 128), F32),
            pltpu.VMEM((8, ROWS, 256), BF),
            pltpu.VMEM((ROWS, 128), F32),
            pltpu.VMEM((2, ROWS, 512), F32),
            pltpu.VMEM((ROWS, 1024), BF),
            pltpu.VMEM((2, 4, ROWS, 256), BF),
            pltpu.VMEM((4, ROWS, 256), BF),
            pltpu.VMEM((2, 512, 256), BF),
            pltpu.VMEM((2, 512, 256), BF),
            pltpu.SemaphoreType.DMA((4,)),
            pltpu.SemaphoreType.DMA((5,)),
            pltpu.SemaphoreType.DMA((2, 29)),
            pltpu.SemaphoreType.DMA((7,)),
            pltpu.SemaphoreType.DMA((4, 2)),
            pltpu.SemaphoreType.DMA((5,)),
        ],
        compiler_params=pltpu.CompilerParams(collective_id=0, has_side_effects=True, vmem_limit_bytes=40 << 20),
    )(in_hbm(tokens), in_hbm(norm_gain.reshape(1, 128)), in_hbm(up_master), in_hbm(down_master))
    return pl.pallas_call(
        put_out,
        name="put_out",
        out_shape=(
            jax.ShapeDtypeStruct((D, 1024), BF),
            jax.ShapeDtypeStruct((1024, D), BF),
            jax.ShapeDtypeStruct((ROWS, 256), BF),
        ),
        in_specs=[vmem] * 4,
        out_specs=(anywhere,) * 3,
        scratch_shapes=[pltpu.VMEM((ROWS, 256), BF), pltpu.SemaphoreType.DMA((33,))],
        compiler_params=pltpu.CompilerParams(vmem_limit_bytes=16 << 20),
    )(*held)


def solution(mesh):
    in_specs = (P("fs", "tp"), P("fs"), P("fs", "tp"), P("fs", "tp"))
    out_specs = (P(None, "tp"), P("tp", None), P("fs", "tp"))
    return jax.shard_map(
        on_device, mesh=mesh, in_specs=in_specs, out_specs=out_specs, check_vma=False
    )
```

```python
import jax
import jax.numpy as jnp
from jax import lax
from jax.experimental import pallas as pl
from jax.experimental.pallas import tpu as pltpu
from jax.sharding import PartitionSpec as P

norm_floor = 1e-06

MESH = pl.DeviceIdType.MESH
BF, F32 = jnp.bfloat16, jnp.float32
D, FF = 2048, 8192
ROWS = 1024
TILE = 512
UP, DN = 0, 1
GROUPS = (
    [(0, j, "G", s) for j in (0, "+") for s in (1, -1)],
    [(1, 0, "G", s) for s in ("+", "-")],
    [(0, 2, "T", 1, 1), (0, 2, "T", -1, 0)] + [(1, j, "G", s) for j in (1, -1) for s in ("+", "-")],
    [(0, j, "G", s) for j in ("-", 2) for s in (1, -1)] + [(1, 2, "T", "-", 0), (1, 2, "G", "+"), (1, 2, "G", "-")],
)


def kernel(
    tok_in, gain_in, up_in, dn_in,
    up_v, dn_v, out_v,
    up32, dn32, gain_v, tok_v, scale_v, acc, hid, pbuf, prx, fwd, qf, fin,
    in_sem, sent_sem, w_recv, t_recv, p_recv, r_recv,
):
    fs, tp = lax.axis_index("fs"), lax.axis_index("tp")
    z, y, x, c = fs // 4, fs % 4, tp // 2, tp % 2
    mod4 = lambda v: lax.rem(v + 8, 4)
    to_y = lambda s: {"fs": z * 4 + mod4(y + s), "tp": tp}
    to_z = lambda s: {"fs": mod4(z + s) * 4 + y, "tp": tp}
    to_x = lambda s: {"fs": fs, "tp": mod4(x + s) * 2 + c}
    partner = {"fs": fs, "tp": x * 2 + 1 - c}

    loads = [
        pltpu.make_async_copy(up_in, up32, in_sem.at[0]),
        pltpu.make_async_copy(gain_in, gain_v, in_sem.at[1]),
        pltpu.make_async_copy(tok_in, tok_v.at[tp], in_sem.at[2]),
        pltpu.make_async_copy(dn_in, dn32, in_sem.at[3]),
    ]
    loads[0].start()
    loads[1].start()
    barrier = pltpu.get_barrier_semaphore()
    for peer in (to_y(1), to_y(-1), to_z(1), to_z(-1), to_x(1), to_x(-1), partner):
        pl.semaphore_signal(barrier, inc=1, device_id=peer, device_id_type=MESH)

    def remote(src, dst, landed, send_sem, recv_sem, peer):
        out = lambda: pltpu.make_async_remote_copy(src, dst, send_sem, recv_sem, peer, MESH)
        back = lambda: pltpu.make_async_remote_copy(landed, landed, send_sem, recv_sem, peer, MESH)
        return out, back

    def go(pair):
        pair[0]().start()

    toward = 1 - 2 * (y % 2)
    y_at = {0: 0, "+": toward, "-": -toward, 2: 2}

    def weight_copies(w):
        def piece(h, jy, jz, q):
            f = mod4(z + jz) * 4 + mod4(y + y_at[jy])
            if w == UP:
                at, n = f * 128 + (0 if q is None else 64 * q), 128 if q is None else 64
                return up_v.at[h, pl.ds(pl.multiple_of(at, 64), n)]
            at, n = 512 * h + (0 if q is None else 256 * q), 512 if q is None else 256
            return dn_v.at[f, pl.ds(at, n)]

        tables, single = ({}, {}), [len(GROUPS)]

        def add(h, name, sent, side, landed):
            group = [g for g, names in enumerate(GROUPS) if (h, *name) in names]
            k = group[0] if group else single[0]
            single[0] += not group
            peer = to_y(y_at[side]) if side in ("+", "-") else to_z(side)
            src, got = piece(h, *sent), piece(h, *landed)
            tables[h][name] = remote(src, src, got, sent_sem.at[w], w_recv.at[w, k], peer)

        for s, other, q in (("+", "-", 1), ("-", "+", 0)):
            add(0, ("S", s), (0, 0, None), s, (s, 0, None))
            add(0, ("F", s), (other, 0, q), s, (2, 0, q))
            for jz in (0, 1, -1):
                add(1, (jz, "T", s), (0, jz, None), s, (s, jz, None))
                add(1, (jz, "G", s), (other, jz, q), s, (2, jz, q))
            for part in (0, 1):
                add(1, (2, "T", s, part), (0, 2, part), s, (s, 2, part))
            add(1, (2, "G", s), (other, 2, q), s, (2, 2, q))
        for s, q in ((1, 0), (-1, 1)):
            add(1, ("S", s), (0, 0, None), s, (0, -s, None))
            add(1, ("F", s), (0, -s, q), s, (0, 2, q))
            for jy in (0, "+", "-"):
                add(0, (jy, "T", s), (jy, 0, None), s, (jy, -s, None))
                add(0, (jy, "G", s), (jy, -s, q), s, (jy, 2, q))
            for part in (0, 1):
                add(0, (2, "T", s, part), (2, 0, part), s, (2, -s, part))
            add(0, (2, "G", s), (2, -s, q), s, (2, 2, q))
        return tables

    W = [weight_copies(w) for w in (UP, DN)]

    def take(w, h, *names):
        for name in names:
            W[w][h][name][1]().wait_recv()

    def take_group(w, g):
        n = len(GROUPS[g])
        if w == UP:
            ref = up_v.at[0, pl.ds(0, 64 * n)]
        else:
            ref = dn_v.at[pl.ds(0, n), pl.ds(0, 256)]
        pltpu.make_async_copy(ref, ref, w_recv.at[w, g]).wait()

    def put(w, h, *names):
        for name in names:
            go(W[w][h][name])

    def e0y(w):
        put(w, 0, ("S", "+"), ("S", "-"))
        put(w, 1, (0, "T", "+"), (0, "T", "-"))

    def e0z(w):
        put(w, 1, ("S", 1), ("S", -1))
        put(w, 0, (0, "T", 1), (0, "T", -1))

    def e1(w):
        take(w, 0, ("S", "+"))
        put(w, 0, ("+", "T", 1), ("+", "T", -1), ("F", "-"))
        for s in (1, -1):
            take(w, 1, ("S", s))
            put(w, 1, (-s, "T", "+"), (-s, "T", "-"), ("F", s))
        take(w, 0, ("S", "-"))
        put(w, 0, ("F", "+"))

    def e2(w):
        for s in (1, -1):
            take(w, 0, (0, "T", s))
            put(w, 0, (0, "G", s))
        take(w, 1, (0, "T", "+"))
        put(w, 1, (0, "G", "-"))
        take(w, 1, (0, "T", "-"))

    def e3a(w):
        for s in (1, -1):
            take(w, 0, ("+", "T", s))
            put(w, 0, ("+", "G", s))

    def e3b(w):
        for s, q in ((1, 0), (-1, 1)):
            take(w, 1, ("F", s))
            put(w, 1, (2, "T", "+", q), (2, "T", "-", q))
        put(w, 0, ("-", "T", 1), ("-", "T", -1))
        put(w, 1, (0, "G", "+"))

    def e3c(w):
        for s, q in (("-", 0), ("+", 1)):
            take(w, 0, ("F", s))
            put(w, 0, (2, "T", 1, q), (2, "T", -1, q))

    def e4a(w, sides=(-1, 1)):
        for jz in sides:
            for s, other in (("+", "-"), ("-", "+")):
                take(w, 1, (jz, "T", s))
                put(w, 1, (jz, "G", other))

    def own_far(w):
        take_group(w, 0)
        take(w, 1, (2, "T", "+", 0))
        put(w, 1, (2, "G", "-"))
        take(w, 1, (2, "T", "+", 1))

    def e4b(w):
        take(w, 1, (2, "T", "-", 1))
        put(w, 1, (2, "G", "+"))

    def e4c(w):
        for s in (1, -1):
            take(w, 0, ("-", "T", s))
            put(w, 0, ("-", "G", s))

    def e4d(w):
        for s, q in ((1, 0), (-1, 1)):
            take(w, 0, (2, "T", s, q))
            put(w, 0, (2, "G", s))

    def other_near(w):
        take_group(w, 1)

    def other_side(w):
        take_group(w, 2)

    def other_far(w):
        take_group(w, 3)

    def rows_of(t, half):
        return tok_v.at[t] if half is None else tok_v.at[t, pl.ds(512 * half, 512)]

    block = lambda d, core: mod4(x + d) * 2 + core
    T = {}

    def token_copy(name, d_sent, half, peer, d_landed, core_landed):
        k = min(len(T), 6)
        sent, got = rows_of(block(d_sent, c), half), rows_of(block(d_landed, core_landed), half)
        T[name] = remote(sent, sent, got, sent_sem.at[2], t_recv.at[k], peer)

    for half in (0, 1):
        token_copy(("X+", half), 0, half, to_x(1), -1, c)
        token_copy(("X-", half), 0, half, to_x(-1), 1, c)
    token_copy("Y+", -1, 0, to_x(1), 2, c)
    token_copy("Y-", 1, 1, to_x(-1), 2, c)
    token_copy(("D", 0), 0, None, partner, 0, 1 - c)
    token_copy(("D", -1), -1, None, partner, -1, 1 - c)
    token_copy(("D", 1), 1, None, partner, 1, 1 - c)
    token_copy(("D", 2, 0), 2, 0, partner, 2, 1 - c)
    token_copy(("D", 2, 1), 2, 1, partner, 2, 1 - c)

    loads[0].wait()
    loads[2].start()
    loads[3].start()
    loads[1].wait()
    gain = jnp.transpose(jnp.broadcast_to(gain_v[...], (128, 128)))
    for h in (0, 1):
        for k in range(4):
            cols = slice(512 * h + 128 * k, 512 * h + 128 * k + 128)
            up_v[h, pl.ds(pl.multiple_of(fs * 128, 128), 128), 128 * k : 128 * k + 128] = (gain * up32[:, cols]).astype(BF)
    pl.semaphore_wait(barrier, 7)

    e0y(UP)
    e0z(UP)
    loads[2].wait()
    go(T["X+", 0]), go(T["X-", 1]), go(T["X+", 1]), go(T["X-", 0])
    go(T["D", 0])

    loads[3].wait()
    for k in range(8):
        dn_v[fs, 128 * k : 128 * k + 128, :] = jnp.transpose(dn32[:, 128 * k : 128 * k + 128]).astype(BF)

    e1(UP)
    e2(UP)
    T["X+", 0][1]().wait_recv()
    go(T["Y+"])
    T["X-", 1][1]().wait_recv()
    go(T["Y-"])
    e3a(UP)
    e3b(UP)
    T["X+", 1][1]().wait_recv()
    go(T["D", -1])
    T["X-", 0][1]().wait_recv()
    go(T["D", 1])
    e4a(UP)
    e3c(UP)
    e4c(UP)
    own_far(UP)
    T["Y+"][1]().wait_recv()
    go(T["D", 2, 0])
    T["Y-"][1]().wait_recv()
    go(T["D", 2, 1])
    e4b(UP)
    e0y(DN)
    e4d(UP)
    e0z(DN)
    pltpu.make_async_copy(tok_v.at[pl.ds(0, 4)], tok_v.at[pl.ds(0, 4)], t_recv.at[6]).wait()

    ones = jnp.ones((128, 128), BF)

    def factor(m, carry):
        rows = pl.ds(pl.multiple_of(m * 256, 256), 256)
        total = jnp.zeros((256, 128), F32)
        for t in range(8):
            v = tok_v[t, rows, :].astype(F32)
            total += v[:, :128] * v[:, :128] + v[:, 128:] * v[:, 128:]
        high = total.astype(BF)
        low = (total - high.astype(F32)).astype(BF)
        summed = jnp.dot(high, ones, preferred_element_type=F32) + jnp.dot(low, ones, preferred_element_type=F32)
        scale_v[rows, :] = lax.rsqrt(summed * (1.0 / D) + norm_floor)
        return carry

    lax.fori_loop(0, ROWS // 256, factor, 0)

    near = y // 2

    def core_of(o):
        return near if o == 0 else 1 - near

    def pair_of(dz, o):
        return mod4(z + dz) * 2 + core_of(o)

    def dots(h, rows, pairs):
        total = None
        for pair in pairs:
            t = pair_of(*pair)
            weights = up_v[h, pl.ds(pl.multiple_of(256 * t, 256), 256), :]
            term = jnp.dot(tok_v[t, rows, :], weights, preferred_element_type=F32)
            total = term if total is None else total + term
        return total

    def first_part(i, carry):
        h, m = i // (ROWS // TILE), lax.rem(i, ROWS // TILE)
        rows = pl.ds(pl.multiple_of(m * TILE, TILE), TILE)
        acc[h, rows, :] = dots(h, rows, ((0, 0), (1, 0), (3, 0), (2, 0)))
        return carry

    def second_part(h):
        def tile(m, carry):
            rows = pl.ds(pl.multiple_of(m * TILE, TILE), TILE)
            total = acc[h, rows, :] + dots(h, rows, ((0, 1), (1, 1), (3, 1), (2, 1)))
            factor_of = scale_v[rows, :]
            for k in range(4):
                v = jnp.maximum(total[:, 128 * k : 128 * k + 128] * factor_of, 0.0)
                hid[rows, 512 * h + 128 * k : 512 * h + 128 * k + 128] = (v * v).astype(BF)
            return carry

        lax.fori_loop(0, ROWS // TILE, tile, 0)

    lax.fori_loop(0, 2 * ROWS // TILE, first_part, 0)
    other_near(UP)
    other_side(UP)
    other_far(UP)
    second_part(0)
    e1(DN)
    second_part(1)
    e2(DN)

    def remote_partial(dz, o, r):
        part = pl.ds(pl.multiple_of(512 * r, 512), 512)
        return remote(pbuf.at[o, dz, part], prx.at[dz, part], prx.at[dz, part], sent_sem.at[3], p_recv.at[dz, r], partner)

    def product(dz, o):
        t = pair_of(dz, o)

        def tile(r, carry):
            rows = pl.ds(pl.multiple_of(r * 512, 512), 512)
            pair = jnp.concatenate([dn_v[2 * t], dn_v[2 * t + 1]], axis=1)
            pbuf[o, dz, rows, :] = jnp.dot(hid[rows, :], pair, preferred_element_type=F32).astype(BF)

            @pl.when(core_of(o) != c)
            def _():
                remote_partial(dz, o, r)[0]().start()

            return carry

        lax.fori_loop(0, 2, tile, 0)

    def ring(sign):
        side = 0 if sign == 1 else 1
        q, k, peer = side, 2 * side, to_x(sign)
        chunk = lambda ref, base, j: ref.at[pl.ds(base + 256 * j, 256)]

        def first(src, j):
            got = chunk(fwd.at[side], 0, j)
            return remote(chunk(src, 512 * q, j), got, got, sent_sem.at[4], r_recv.at[k + j], peer)

        def second(j):
            got = chunk(fin.at[side], 512 * q, j)
            return remote(chunk(qf.at[side], 0, j), got, got, sent_sem.at[4], r_recv.at[4], peer)

        def direct(src, j):
            got = chunk(fin.at[side], 512 * (1 - q), j)
            return remote(chunk(src, 512 * (1 - q), j), got, got, sent_sem.at[4], r_recv.at[4], peer)

        return first, second, direct

    RING = {1: ring(1), -1: ring(-1)}
    ahead = lambda dz: mod4(z + dz - x)

    def reduce_pair(dz, o):
        @pl.when(core_of(o) == c)
        def _():
            mine = pbuf.at[o, dz]
            for r, sign, d in ((0, 1, 3), (1, -1, 1)):
                remote_partial(dz, o, r)[1]().wait_recv()
                rows = pl.ds(512 * r, 512)
                pbuf[o, dz, rows, :] = (pbuf[o, dz, rows, :].astype(F32) + prx[dz, rows, :].astype(F32)).astype(BF)

                @pl.when(ahead(dz) == 2)
                def _():
                    RING[sign][0](mine, 0)[0]().start()
                    RING[sign][0](mine, 1)[0]().start()

                @pl.when(ahead(dz) == d)
                def _():
                    RING[-sign][2](mine, 0)[0]().start()
                    if not later(dz, o):
                        RING[-sign][2](mine, 1)[0]().start()

    later = lambda dz, o: o == 1 and dz in (1, 3)

    def direct_rest(dz, o):
        @pl.when(core_of(o) == c)
        def _():
            for sign, d in ((1, 1), (-1, 3)):
                @pl.when(ahead(dz) == d)
                def _():
                    RING[sign][2](pbuf.at[o, dz], 1)[0]().start()

    def forward(dz, o):
        @pl.when(core_of(o) == c)
        def _():
            for sign, d in ((1, 1), (-1, 3)):
                side = 0 if sign == 1 else 1

                @pl.when(ahead(dz) == d)
                def _():
                    for j in (0, 1):
                        RING[sign][0](pbuf.at[o, dz], j)[1]().wait_recv()
                        here, mine = pl.ds(256 * j, 256), pl.ds(512 * side + 256 * j, 256)
                        qf[side, here, :] = (pbuf[o, dz, mine, :].astype(F32) + fwd[side, here, :].astype(F32)).astype(BF)
                        RING[sign][1](j)[0]().start()

    product(0, 0)
    reduce_pair(0, 0)
    e3a(DN)
    e4a(DN, (-1,))
    product(3, 0)
    e3b(DN)
    reduce_pair(3, 0)
    forward(0, 0)
    e4a(DN, (1,))
    product(1, 0)
    e3c(DN)
    reduce_pair(1, 0)
    own_far(DN)
    product(2, 0)
    e4c(DN)
    reduce_pair(2, 0)
    e4b(DN)
    forward(3, 0)
    other_near(DN)
    product(0, 1)
    e4d(DN)
    other_side(DN)
    product(1, 1)
    reduce_pair(0, 1)
    product(3, 1)
    forward(1, 0)
    reduce_pair(1, 1)
    reduce_pair(3, 1)
    other_far(DN)
    product(2, 1)
    forward(2, 0)
    reduce_pair(2, 1)
    direct_rest(1, 1)
    direct_rest(3, 1)
    forward(0, 1)
    forward(1, 1)
    forward(3, 1)
    forward(2, 1)

    mine = mod4(x - z)
    o_mine = jnp.where(near == c, 0, 1)
    pltpu.make_async_copy(fin, fin, r_recv.at[4]).wait()

    def last(m, carry):
        rows = pl.ds(pl.multiple_of(m * TILE, TILE), TILE)
        total = pbuf[o_mine, mine, rows, :].astype(F32) + fin[0, rows, :].astype(F32) + fin[1, rows, :].astype(F32)
        out_v[rows, :] = total.astype(BF)
        return carry

    lax.fori_loop(0, ROWS // TILE, last, 0)

    for k, ref in enumerate((up_v.at[:, pl.ds(0, 1920)], dn_v.at[pl.ds(0, 15)], tok_v.at[pl.ds(0, 7)], prx, pbuf.at[0, pl.ds(0, 3)])):
        pltpu.make_async_copy(ref, ref, sent_sem.at[k]).wait()


def put_out(up_v, dn_v, out_v, up_out, dn_out, out, sem):
    copies = [pltpu.make_async_copy(out_v, out, sem.at[32])]
    for f in range(16):
        copies.append(pltpu.make_async_copy(dn_v.at[f], dn_out.at[:, pl.ds(128 * f, 128)], sem.at[f]))
    for k in range(16):
        rows, h = pl.ds(256 * (k // 2), 256), k % 2
        copies.append(pltpu.make_async_copy(up_v.at[h, rows], up_out.at[rows, pl.ds(512 * h, 512)], sem.at[16 + k]))
    for copy in copies:
        copy.start()
    for copy in copies:
        copy.wait()


def on_device(tokens, norm_gain, up_master, down_master):
    anywhere, vmem = pl.BlockSpec(memory_space=pl.ANY), pl.BlockSpec(memory_space=pltpu.VMEM)
    in_hbm = lambda v: pltpu.with_memory_space_constraint(v, pltpu.HBM)
    held = pl.pallas_call(
        kernel,
        name="gather_mlp",
        out_shape=(
            pltpu.VMEM((2, D, 512), BF),
            pltpu.VMEM((16, 1024, 128), BF),
            pltpu.VMEM((ROWS, 256), BF),
        ),
        in_specs=[anywhere] * 4,
        out_specs=(vmem, vmem, vmem),
        scratch_shapes=[
            pltpu.VMEM((128, 1024), F32),
            pltpu.VMEM((128, 1024), F32),
            pltpu.VMEM((1, 128), F32),
            pltpu.VMEM((8, ROWS, 256), BF),
            pltpu.VMEM((ROWS, 128), F32),
            pltpu.VMEM((2, ROWS, 512), F32),
            pltpu.VMEM((ROWS, 1024), BF),
            pltpu.VMEM((2, 4, ROWS, 256), BF),
            pltpu.VMEM((4, ROWS, 256), BF),
            pltpu.VMEM((2, 512, 256), BF),
            pltpu.VMEM((2, 512, 256), BF),
            pltpu.VMEM((2, ROWS, 256), BF),
            pltpu.SemaphoreType.DMA((4,)),
            pltpu.SemaphoreType.DMA((5,)),
            pltpu.SemaphoreType.DMA((2, 29)),
            pltpu.SemaphoreType.DMA((7,)),
            pltpu.SemaphoreType.DMA((4, 2)),
            pltpu.SemaphoreType.DMA((5,)),
        ],
        compiler_params=pltpu.CompilerParams(collective_id=0, has_side_effects=True, vmem_limit_bytes=40 << 20),
    )(in_hbm(tokens), in_hbm(norm_gain.reshape(1, 128)), in_hbm(up_master), in_hbm(down_master))
    return pl.pallas_call(
        put_out,
        name="put_out",
        out_shape=(
            jax.ShapeDtypeStruct((D, 1024), BF),
            jax.ShapeDtypeStruct((1024, D), BF),
            jax.ShapeDtypeStruct((ROWS, 256), BF),
        ),
        in_specs=[vmem] * 3,
        out_specs=(anywhere,) * 3,
        scratch_shapes=[pltpu.SemaphoreType.DMA((33,))],
        compiler_params=pltpu.CompilerParams(vmem_limit_bytes=16 << 20),
    )(*held)


def solution(mesh):
    in_specs = (P("fs", "tp"), P("fs"), P("fs", "tp"), P("fs", "tp"))
    out_specs = (P(None, "tp"), P("tp", None), P("fs", "tp"))
    return jax.shard_map(
        on_device, mesh=mesh, in_specs=in_specs, out_specs=out_specs, check_vma=False
    )
```
